1024 devices in a mesh: fs: 256 (over z, y, core), tp: 4 (over x).
Axes of the slice: x: 4, y: 8, z: 16, core: 2. Of those that a mesh axis runs over, the one named last changes fastest.
Arguments:
- inputs: bfloat16 [524288, 2048], P('fs'), may hold values from -24 to 24
- key_grads: bfloat16 [524288, 1024], P('fs', 'tp'), may hold values from -0.01953125 to 0.01953125
- weights: float32 [2048, 1024], P('fs', 'tp'), may hold values from -6 to 6
- momentum: float32 [2048, 1024], P('fs', 'tp'), may hold values from -6 to 6
- left_stat: float32 [4, 2048, 2048], P('tp', 'fs'), may hold values from -96 to 96
- right_stat: float32 [8, 128, 128], P('tp'), may hold values from -256 to 256
- left_root: bfloat16 [4, 2048, 2048], P('tp', 'fs'), may hold values from -0.125 to 0.125
- right_root: bfloat16 [8, 128, 128], P('tp'), may hold values from -0.5 to 0.5
Outputs:
- momentum_next: float32 [2048, 1024], P('fs', 'tp')
- left_next: float32 [4, 2048, 2048], P('tp', 'fs')
- right_next: float32 [8, 128, 128], P('tp')
- update: float32 [2048, 1024], P('fs', 'tp')
- weights_next: float32 [2048, 1024], P('fs', 'tp')
- weights_copy: bfloat16 [2048, 1024], P(None, 'tp')
The draws below stay inside these ranges and needn't reach their ends.
All inputs are finite; a program needn't handle non-finite values.
Results may differ from the reference program's by a relative error of at most 0.0033.
Values may be sent and summed in bfloat16 or wider, within the bound.
A program may use at most 64 MiB of HBM per device.

```python
import jax
import jax.numpy as jnp
from jax import lax

D = 2048
HEADS = 8
HD = 128
COLBLK = 256
TOKENS = 524288
C = 1024
NBLK = 4


def with_spikes(values, rng, source, target, blocks, factor):
    def block_of(axis_at):
        return (jnp.arange(values.shape[axis_at]) // (values.shape[axis_at] // blocks)).reshape((-1,) + (1,) * (values.ndim - 1 - axis_at))

    one_side = jax.random.permutation(rng, blocks)[block_of(target)]
    second = (block_of(target) + blocks // 2) % blocks
    return jnp.where((block_of(source) == one_side) | (block_of(source) == second), factor * values, values)


def block_scale(rng, extent, cuts, least, largest):
    level, own = 1.0, jax.random.fold_in(rng, 6)
    for position, blocks in cuts:
        draws = jnp.exp(jax.random.uniform(jax.random.fold_in(own, position), (blocks,), jnp.float32, least / len(cuts), largest / len(cuts)))
        level = level * jnp.repeat(draws, extent[position] // blocks).reshape([-1 if axis == position else 1 for axis in range(len(extent))])
    return level


def centred(stream_key, dims, scale, reach, shards=(), kind=jnp.bfloat16):
    gain = block_scale(stream_key, dims, shards, -0.22, 0.18) if shards else 1.0
    array = jax.random.normal(stream_key, dims, jnp.float32) * scale * gain
    return jnp.minimum(jnp.maximum(array, -reach), reach).astype(kind)


def bell_draw_with(stream_key, extent, scale, limit, split, heavy, kind=jnp.bfloat16):
    result = scale * jax.random.normal(stream_key, extent, jnp.float32)
    if split:
        result = result * block_scale(stream_key, extent, split, -0.22, 0.18)
    return jnp.clip(with_spikes(result, jax.random.fold_in(stream_key, 3), *heavy), -limit, limit).astype(kind)


def setup_inputs(seed: int = 0) -> dict:
    key_list = jax.random.split(jax.random.key(seed), 9)
    inputs = bell_draw_with(key_list[0], (TOKENS, D), 1.0, 24.0, ((0, 256),), (0, 1, 256, 6.0))
    key_grads = centred(key_list[1], (TOKENS, C), (TOKENS ** -0.5), 0.01953125, ((0, 256), (1, 4)))
    weights = centred(key_list[2], (D, C), 1.0, 6.0, ((0, 256), (1, 4)), jnp.float32)
    momentum = centred(key_list[3], (D, C), 1.0, 6.0, ((0, 256), (1, 4)), jnp.float32)
    left_stat = centred(key_list[4], (NBLK, D, D), (COLBLK ** 0.5), 96.0, ((0, 4), (1, 256)), jnp.float32)
    right_stat = centred(key_list[5], (HEADS, HD, HD), (D ** 0.5), 256.0, ((0, 4),), jnp.float32)
    left_root = centred(key_list[6], (NBLK, D, D), D ** -0.5, 0.125, ((0, 4), (1, 256)))
    right_root = centred(key_list[7], (HEADS, HD, HD), HD ** -0.5, 0.5, ((0, 4),))
    return {"inputs": inputs, "key_grads": key_grads, "weights": weights, "momentum": momentum, "left_stat": left_stat, "right_stat": right_stat, "left_root": left_root, "right_root": right_root}


def reference(inputs, key_grads, weights, momentum, left_stat, right_stat, left_root, right_root):
    grad = lax.dot_general(inputs, key_grads, (((0,), (0,)), ((), ())), preferred_element_type=jnp.float32)
    grad_bf = grad.astype(jnp.bfloat16)
    nblocks = left_root.shape[0]
    heads = right_root.shape[0]
    head_size = right_root.shape[1]
    width = grad.shape[0]
    blocks = grad_bf.astype(jnp.float32).reshape(width, nblocks, -1)
    left_part = jnp.einsum('brd,dbc->rbc', left_root.astype(jnp.float32), blocks)
    left_part = left_part.reshape(width, -1).astype(jnp.bfloat16)
    precond = jnp.einsum('rhi,hij->rhj', left_part.astype(jnp.float32).reshape(width, heads, head_size), right_root.astype(jnp.float32)).reshape(width, -1)
    left_next = 0.95 * left_stat + 0.05 * jnp.einsum('rbc,sbc->brs', blocks, blocks)
    by_head = grad_bf.astype(jnp.float32).reshape(width, heads, head_size)
    right_next = 0.95 * right_stat + 0.05 * jnp.einsum('rhi,rhj->hij', by_head, by_head)
    scale = jnp.sqrt(jnp.sum(grad * grad) / (jnp.sum(precond * precond) + 1e-06))
    momentum_next = 0.9 * momentum + scale * precond
    update = -0.25 * (momentum_next + 0.4 * weights)
    weights_next = weights + update
    return (momentum_next, left_next, right_next, update, weights_next, weights_next.astype(jnp.bfloat16))
```

```python
import functools

import jax
import jax.numpy as jnp
from jax import lax
from jax.experimental import pallas as pl
from jax.experimental.pallas import tpu as pltpu
from jax.sharding import Mesh
from jax.sharding import PartitionSpec as P

MESH = pl.DeviceIdType.MESH
F32 = jnp.float32
BF16 = jnp.bfloat16
H = 128
ROWS = 16


def offset_of(r, nz):
    half = nz // 2
    if r == 0:
        return half
    return half - (r + 1) // 2 if r % 2 else -(half - r // 2)


def place_of(off, nz):
    half = nz // 2
    if off == 0:
        return nz - 1
    if abs(off) == half:
        return 0
    return 2 * (half - off) - 1 if off > 0 else 2 * (half + off)


def kernel(
    nz, ny, nx, gz,
    x_hbm, k_hbm, w_hbm, m_hbm, ls_hbm, rs_hbm, lr_hbm, rr_hbm,
    mom_hbm, ln_hbm, rn_hbm, up_hbm, wn_hbm, cp_hbm,
    xs, ks, kt, pt, px, sf, ysend, yrecv, zsend, zrecv, gfull, gabs, pfull, afull, ascr, tile, own8, gown,
    wv, mv, lsv, rsv, lrv, rrv, momv, lnv, rnv, upv, wnv, outv,
    sv, s1, s2, s3,
    in_sem, x_sem, out_sem, d_send, d_recv, ry_send, ry_recv, rz_sem, a_sem, ring_send, ring_r, ring_l,
    ag_send, agz_recv, agy_recv, agd_recv, s_send, s_recv,
):
    ng = nz // gz
    blk = ny * ROWS
    z, y, c, x = (lax.axis_index(n) for n in ("z", "y", "c", "x"))
    me = nz - 1
    other = 1 - c
    partner = {"c": other}

    def zpos(off):
        return lax.rem(z + off + nz, nz)

    def ypos(dy):
        return lax.rem(y + dy, ny)

    def send(src, dst, s, r, dev):
        pltpu.make_async_remote_copy(src, dst, s, r, device_id=dev, device_id_type=MESH).start()

    def await_bytes(ref, sem):
        pltpu.make_async_copy(ref, ref, sem).wait()

    xc_peers = [(dx, dc) for dx in range(nx) for dc in range(2) if dx or dc]

    def xc_dev(dx, dc):
        return {"x": lax.rem(x + dx, nx), "c": lax.rem(c + dc, 2)}

    bar = pltpu.get_barrier_semaphore()

    @pl.loop(1, ny)
    def _(dy):
        pl.semaphore_signal(bar, inc=1, device_id={"y": ypos(dy)}, device_id_type=MESH)

    @pl.loop(1, nz)
    def _(dz):
        pl.semaphore_signal(bar, inc=1, device_id={"z": lax.rem(z + dz, nz)}, device_id_type=MESH)

    for dx, dc in xc_peers:
        pl.semaphore_signal(bar, inc=1, device_id=xc_dev(dx, dc), device_id_type=MESH)

    def load(src, dst, i):
        pltpu.make_async_copy(src, dst, in_sem.at[i]).start()

    def loaded(dst, i):
        await_bytes(dst, in_sem.at[i])

    load(k_hbm, ks, 0)
    for r in range(nz):
        src = x_hbm.at[:, pl.ds(pl.multiple_of(zpos(offset_of(r, nz)) * blk, blk), blk)]
        pltpu.make_async_copy(src, xs.at[r // gz, :, pl.ds((r % gz) * blk, blk)], x_sem.at[r // gz]).start()
    load(w_hbm, wv, 1)
    load(m_hbm, mv, 2)
    load(lr_hbm.at[0], lrv.at[c], 3)
    load(rr_hbm, rrv, 4)
    load(ls_hbm.at[0], lsv, 5)
    load(rs_hbm, rsv, 6)

    loaded(ks, 0)
    kt[...] = ks[...].T
    for g in range(ng):
        await_bytes(xs.at[g], x_sem.at[g])
        out = jnp.dot(kt[...], xs[g], preferred_element_type=F32)
        for i in range(gz):
            for h in range(2):
                pt[g, h, i] = out[h * H:(h + 1) * H, i * blk:(i + 1) * blk]

    loaded(wv, 1)
    loaded(mv, 2)
    base = 0.9 * wv[...] - 0.225 * mv[...]
    ascr[0] = base[:, :H]
    ascr[1] = base[:, H:]
    afull[c, me, y, pl.ds(pl.multiple_of(8 * c, 8), 8)] = ascr[c]
    loaded(lrv.at[c], 3)

    pl.semaphore_wait(bar, (ny - 1) + (nz - 1) + len(xc_peers))

    for g in range(ng):
        send(pt.at[g, other], px.at[g], d_send.at[0], d_recv.at[g], partner)
    send(ascr.at[other], afull.at[other, me, y, pl.ds(pl.multiple_of(8 * c, 8), 8)], d_send.at[1], d_recv.at[ng], partner)
    send(lrv.at[c], lrv.at[c], d_send.at[2], d_recv.at[ng + 1], partner)

    for g in range(ng):
        await_bytes(px.at[g], d_recv.at[g])
        for i in range(gz):
            r = g * gz + i
            t = (pt[g, c, i] + px[g, i]).T.reshape(ny, ROWS, H)
            sf[r] = t
            ysend[:, r] = t.astype(BF16)

        @pl.loop(1, ny)
        def _(dy):
            yt = ypos(dy)
            send(ysend.at[yt, pl.ds(g * gz, gz)], yrecv.at[dy - 1, pl.ds(g * gz, gz)], ry_send, ry_recv.at[g], {"y": yt})

        if g == 0:
            await_bytes(ascr.at[0], d_recv.at[ng])

            @pl.loop(1, ny)
            def _(dy):
                send(afull.at[c, me, y], afull.at[c, me, y], a_sem.at[0], a_sem.at[1], {"y": ypos(dy)})

    half = nz // 2

    def ring_step(k):
        if k == 1:
            await_bytes(afull.at[c, me, pl.ds(0, ny - 1)], a_sem.at[1])
        else:
            await_bytes(afull.at[c, 0], ring_r.at[k - 2])
            if k <= half:
                await_bytes(afull.at[c, 0], ring_l.at[k - 2])
        if k <= half:
            src, dst = place_of(-(k - 1), nz), place_of(-k, nz)
            send(afull.at[c, src], afull.at[c, dst], ring_send.at[0], ring_r.at[k - 1], {"z": zpos(1)})
        if k < half:
            src, dst = place_of(k - 1, nz), place_of(k, nz)
            send(afull.at[c, src], afull.at[c, dst], ring_send.at[1], ring_l.at[k - 1], {"z": zpos(-1)})

    steps = iter(range(1, half + 2))

    def ring(n):
        for _ in range(n):
            k = next(steps, None)
            if k is None:
                return
            if k == half + 1:
                await_bytes(afull.at[c, 0], ring_r.at[half - 1])
                send(afull.at[c], afull.at[c], d_send.at[3], d_recv.at[ng + 2], partner)
            else:
                ring_step(k)

    ring(1)
    for g in range(ng):
        await_bytes(yrecv.at[:, pl.ds(g * gz, gz)], ry_recv.at[g])
        for i in range(gz):
            r = g * gz + i
            t = sf[r, y]
            for j in range(ny - 1):
                t = t + yrecv[j, r].astype(F32)
            zsend[r] = t
            if r != me:
                off = offset_of(r, nz)
                back = place_of(-off, nz)
                send(zsend.at[r], zrecv.at[back], rz_sem.at[0], rz_sem.at[1], {"z": zpos(off)})
        if g in (1, 3):
            ring(1)

    await_bytes(zrecv, rz_sem.at[1])
    grad = zsend[me]
    for r in range(nz - 1):
        grad = grad + zrecv[r]
    sv[0:1] = jnp.sum(grad * grad, axis=0, keepdims=True)
    gfull[c, me, y] = grad.astype(BF16)

    groups = [(me, 1)] + [(r, 2) for r in range(nz - 3, 0, -2)] + [(0, 1)]

    def gather_start(full, p):
        for r in range(nz - 1):
            off = offset_of(r, nz)
            back = place_of(-off, nz)
            j = [q for q, (r0, n) in enumerate(groups) if r0 <= back < r0 + n][0]
            send(full.at[c, me, y], full.at[c, back, y], ag_send.at[p, 0], agz_recv.at[p, j], {"z": zpos(off)})
        gather_forward(full, p, 0)

    def gather_forward(full, p, j):
        r0, n = groups[j]
        if j:
            await_bytes(full.at[c, pl.ds(r0, n), y], agz_recv.at[p, j])

        @pl.loop(1, ny)
        def _(dy):
            slab = full.at[c, pl.ds(r0, n), y]
            send(slab, slab, ag_send.at[p, 1], agy_recv.at[p, j], {"y": ypos(dy)})

    def gather_land(full, p, j):
        r0, n = groups[j]
        await_bytes(full.at[c, pl.ds(r0, n), pl.ds(0, ny - 1)], agy_recv.at[p, j])
        slab = full.at[c, pl.ds(r0, n)]
        send(slab, slab, ag_send.at[p, 2], agd_recv.at[p, j], partner)

    def gather_close(full, p):
        await_bytes(full.at[0, pl.ds(0, nz - 1), 0], ag_send.at[p, 0])
        await_bytes(full.at[0, :, pl.ds(0, ny - 1)], ag_send.at[p, 1])
        await_bytes(full.at[0], ag_send.at[p, 2])

    gather_start(gfull, 0)
    ring(1)
    for j in range(1, len(groups)):
        gather_forward(gfull, 0, j)
    ring(1)

    def keep(h, j):
        r0, n = groups[j]
        for r in range(r0, r0 + n):
            gabs[h, pl.ds(pl.multiple_of(zpos(offset_of(r, nz)) * blk, blk), blk)] = gfull[h, r].reshape(blk, H)

    for j in range(len(groups)):
        gather_land(gfull, 0, j)
        keep(c, j)

    await_bytes(lrv.at[0], d_recv.at[ng + 1])
    loaded(rrv, 4)
    lm = jnp.concatenate([lrv[0].astype(F32), lrv[1].astype(F32)], axis=0).astype(BF16)
    left = jnp.dot(lm, gabs[c], preferred_element_type=F32)
    hi = left.astype(BF16)
    lo = (left - hi.astype(F32)).astype(BF16)
    rr = rrv[c]
    pre = jnp.dot(hi, rr, preferred_element_type=F32) + jnp.dot(lo, rr, preferred_element_type=F32)
    pfull[c, me, y] = pre.astype(BF16)
    gather_start(pfull, 1)
    sv[1:2] = jnp.sum(pre * pre, axis=0, keepdims=True)
    tile[...] = pre

    s1[x * 2 + c] = sv[...]
    for dx, dc in xc_peers:
        send(sv, s1.at[x * 2 + c], s_send.at[0], s_recv.at[0], xc_dev(dx, dc))
    send(tile.at[pl.ds(pl.multiple_of(8 * other, 8), 8)], own8.at[c], d_send.at[4], d_recv.at[ng + 3], partner)
    own8[c] = tile[pl.ds(pl.multiple_of(8 * c, 8), 8)]
    ring(1)

    for j in range(len(groups)):
        r0, n = groups[j]
        await_bytes(gfull.at[other, pl.ds(r0, n)], agd_recv.at[0, j])
        keep(other, j)
    gram = None
    for h in range(2):
        gown[...] = gfull[h, me, y].astype(F32)
        mine = gown[pl.ds(pl.multiple_of(8 * c, 8), 8)].astype(BF16)
        part = lax.dot_general(mine, gabs[h], (((1,), (1,)), ((), ())), preferred_element_type=F32)
        gram = part if gram is None else gram + part
    loaded(lsv, 5)
    lnv[...] = 0.95 * lsv[...] + 0.05 * gram
    pltpu.make_async_copy(lnv, ln_hbm.at[0], out_sem.at[0]).start()

    await_bytes(s1.at[pl.ds(0, 2 * nx - 1)], s_recv.at[0])
    tot = s1[0]
    for i in range(1, 2 * nx):
        tot = tot + s1[i]
    s2[z] = tot

    @pl.loop(1, nz)
    def _(dz):
        send(s2.at[z], s2.at[z], s_send.at[1], s_recv.at[1], {"z": lax.rem(z + dz, nz)})

    for j in range(1, len(groups)):
        gather_forward(pfull, 1, j)

    loaded(rsv, 6)
    for h in range(2):
        gh = gabs[h]
        hg = lax.dot_general(gh, gh, (((0,), (0,)), ((), ())), preferred_element_type=F32)
        rnv[h] = 0.95 * rsv[h] + 0.05 * hg
    pltpu.make_async_copy(rnv, rn_hbm, out_sem.at[1]).start()

    await_bytes(s2.at[pl.ds(0, nz - 1)], s_recv.at[1])
    tot = s2[0]
    for i in range(1, nz):
        tot = tot + s2[i]
    s3[y] = tot

    @pl.loop(1, ny)
    def _(dy):
        send(s3.at[y], s3.at[y], s_send.at[2], s_recv.at[2], {"y": ypos(dy)})

    ring(nz)
    for j in range(len(groups)):
        gather_land(pfull, 1, j)

    await_bytes(s3.at[pl.ds(0, ny - 1)], s_recv.at[2])
    tot = s3[0]
    for i in range(1, ny):
        tot = tot + s3[i]
    gs = jnp.sum(tot[0:1], axis=1, keepdims=True)
    ps = jnp.sum(tot[1:2], axis=1, keepdims=True)
    scale = jnp.sqrt(gs / (ps + 1e-06))

    await_bytes(own8.at[0], d_recv.at[ng + 3])
    wide = jnp.concatenate([own8[0], own8[1]], axis=1)
    mom = 0.9 * mv[...] + scale * wide
    upd = -0.25 * (mom + 0.4 * wv[...])
    momv[...] = mom
    upv[...] = upd
    wnv[...] = wv[...] + upd
    pltpu.make_async_copy(momv, mom_hbm, out_sem.at[2]).start()
    pltpu.make_async_copy(upv, up_hbm, out_sem.at[3]).start()
    pltpu.make_async_copy(wnv, wn_hbm, out_sem.at[4]).start()

    await_bytes(afull.at[other], d_recv.at[ng + 2])
    quarter = 0.25 * scale
    for j in range(len(groups)):
        r0, n = groups[j]
        await_bytes(pfull.at[other, pl.ds(r0, n)], agd_recv.at[1, j])
        for r in range(r0, r0 + n):
            for h in range(2):
                v = afull[h, r].reshape(blk, H) - quarter * pfull[h, r].reshape(blk, H).astype(F32)
                outv[r, :, h * H:(h + 1) * H] = v.astype(BF16)
            dst = cp_hbm.at[pl.ds(pl.multiple_of(zpos(offset_of(r, nz)) * blk, blk), blk)]
            pltpu.make_async_copy(outv.at[r], dst, out_sem.at[5]).start()

    await_bytes(pt.at[:, 0], d_send.at[0])
    await_bytes(ascr.at[0], d_send.at[1])
    await_bytes(lrv.at[0], d_send.at[2])
    await_bytes(afull.at[0], d_send.at[3])
    await_bytes(own8.at[0], d_send.at[4])
    await_bytes(yrecv, ry_send)
    await_bytes(zrecv, rz_sem.at[0])
    await_bytes(afull.at[0, 0, pl.ds(0, ny - 1)], a_sem.at[0])
    await_bytes(afull.at[0, pl.ds(0, half)], ring_send.at[0])
    if half > 1:
        await_bytes(afull.at[0, pl.ds(0, half - 1)], ring_send.at[1])
    gather_close(gfull, 0)
    gather_close(pfull, 1)
    await_bytes(s1.at[pl.ds(0, 2 * nx - 1)], s_send.at[0])
    await_bytes(s2.at[pl.ds(0, nz - 1)], s_send.at[1])
    await_bytes(s3.at[pl.ds(0, ny - 1)], s_send.at[2])
    await_bytes(lnv, out_sem.at[0])
    await_bytes(rnv, out_sem.at[1])
    await_bytes(momv, out_sem.at[2])
    await_bytes(upv, out_sem.at[3])
    await_bytes(wnv, out_sem.at[4])
    await_bytes(outv, out_sem.at[5])


def body(nz, ny, nx, gz, inputs, key_grads, weights, momentum, left_stat, right_stat, left_root, right_root):
    tokens, width = inputs.shape
    ng, blk, ngr = nz // gz, ny * ROWS, nz // 2 + 1
    dma = pltpu.SemaphoreType.DMA
    v = pltpu.VMEM
    scratch = [
        v((ng, tokens, gz * blk), BF16), v((tokens, 2 * H), BF16), v((2 * H, tokens), BF16),
        v((ng, 2, gz, H, blk), F32), v((ng, gz, H, blk), F32),
        v((nz, ny, ROWS, H), F32), v((ny, nz, ROWS, H), BF16), v((ny - 1, nz, ROWS, H), BF16),
        v((nz, ROWS, H), F32), v((nz - 1, ROWS, H), F32),
        v((2, nz, ny, ROWS, H), BF16), v((2, width, H), BF16), v((2, nz, ny, ROWS, H), BF16), v((2, nz, ny, ROWS, H), F32),
        v((2, 8, H), F32), v((ROWS, H), F32), v((2, 8, H), F32), v((ROWS, H), F32),
        v((8, 2 * H), F32), v((8, 2 * H), F32), v((8, width), F32), v((2, H, H), F32), v((2, 8, width), BF16), v((2, H, H), BF16),
        v((8, 2 * H), F32), v((8, width), F32), v((2, H, H), F32), v((8, 2 * H), F32), v((8, 2 * H), F32),
        v((nz, blk, 2 * H), BF16),
        v((2, H), F32), v((2 * nx, 2, H), F32), v((nz, 2, H), F32), v((ny, 2, H), F32),
        dma((7,)), dma((ng,)), dma((6,)), dma((5,)), dma((ng + 4,)), dma, dma((ng,)), dma((2,)), dma((2,)),
        dma((2,)), dma((nz // 2,)), dma((nz // 2,)),
        dma((2, 3)), dma((2, ngr)), dma((2, ngr)), dma((2, ngr)), dma((3,)), dma((3,)),
    ]
    sds = jax.ShapeDtypeStruct
    anyspace = pl.BlockSpec(memory_space=pl.ANY)
    return pl.pallas_call(
        functools.partial(kernel, nz, ny, nx, gz),
        out_shape=(
            sds(weights.shape, F32), sds(left_stat.shape, F32), sds(right_stat.shape, F32),
            sds(weights.shape, F32), sds(weights.shape, F32), sds((width, 2 * H), BF16),
        ),
        in_specs=[anyspace] * 8,
        out_specs=(anyspace,) * 6,
        scratch_shapes=scratch,
        compiler_params=pltpu.CompilerParams(collective_id=0, has_side_effects=True, vmem_limit_bytes=56 * 2**20),
    )(inputs, key_grads, weights, momentum, left_stat, right_stat, left_root, right_root)


def build(devices, nz, ny, nx, gz):
    split = Mesh(devices.reshape(nz, ny, 2, nx), ("z", "y", "c", "x"))
    fs = ("z", "y", "c")
    in_specs = (
        P(fs, None), P(fs, "x"), P(fs, "x"), P(fs, "x"),
        P("x", fs, None), P("x", None, None), P("x", fs, None), P("x", None, None),
    )
    out_specs = (P(fs, "x"), P("x", fs, None), P("x", None, None), P(fs, "x"), P(fs, "x"), P(None, "x"))
    return jax.shard_map(
        functools.partial(body, nz, ny, nx, gz), mesh=split, in_specs=in_specs, out_specs=out_specs, check_vma=False
    )


def solution(mesh):
    return build(mesh.devices, 16, 8, mesh.shape["tp"], 4)
```

```python
import functools

import jax
import jax.numpy as jnp
from jax import lax
from jax.experimental import pallas as pl
from jax.experimental.pallas import tpu as pltpu
from jax.sharding import Mesh
from jax.sharding import PartitionSpec as P

MESH = pl.DeviceIdType.MESH
F32 = jnp.float32
BF16 = jnp.bfloat16
H = 128
ROWS = 16


def offset_of(r, nz):
    half = nz // 2
    if r == 0:
        return half
    return half - (r + 1) // 2 if r % 2 else -(half - r // 2)


def place_of(off, nz):
    half = nz // 2
    if off == 0:
        return nz - 1
    if abs(off) == half:
        return 0
    return 2 * (half - off) - 1 if off > 0 else 2 * (half + off)


HELD = pltpu.VMEM


def kernel(
    nz, ny, nx, gz,
    x_hbm, k_hbm, w_hbm, m_hbm, ls_hbm, rs_hbm, lr_hbm, rr_hbm,
    momv, lnv, rnv, upv, wnv, outv,
    xs, ks, kt, pt, px, sf, ysend, yrel, ysum, yrecv, zsend, zrecv, gfull, gabs, pfull, afull, ascr, tile, own8, gown,
    wv, mv, lsv, rsv, lrv, rrv,
    sv, s1, s2, s3,
    in_sem, x_sem, d_send, d_recv, ry_send, rel_recv, ry_recv, rz_sem, a_sem, ring_send, ring_r, ring_l,
    ag_send, agz_recv, agx_recv, agy_recv, agd_recv, s_send, s_recv,
):
    ng = nz // gz
    blk = ny * ROWS
    half = nz // 2
    z, y, c, x = (lax.axis_index(n) for n in ("z", "y", "c", "x"))
    me = nz - 1
    other = 1 - c
    sgn = 1 - 2 * c
    partner = {"c": other}
    quad, zi = z // gz, lax.rem(z, gz)
    my8 = pl.ds(pl.multiple_of(8 * c, 8), 8)
    its8 = pl.ds(pl.multiple_of(8 * other, 8), 8)

    def zpos(off):
        return lax.rem(z + off + nz, nz)

    def ypos(dy):
        return lax.rem(y + dy + ny, ny)

    def send(src, dst, s, r, dev):
        pltpu.make_async_remote_copy(src, dst, s, r, device_id=dev, device_id_type=MESH).start()

    def await_bytes(ref, sem):
        pltpu.make_async_copy(ref, ref, sem).wait()

    xc_peers = [(dx, dc) for dx in range(nx) for dc in range(2) if dx or dc]

    def xc_dev(dx, dc):
        return {"x": lax.rem(x + dx, nx), "c": lax.rem(c + dc, 2)}

    def load(src, dst, i):
        pltpu.make_async_copy(src, dst, in_sem.at[i]).start()

    def loaded(dst, i):
        await_bytes(dst, in_sem.at[i])

    quads = [offset_of(r, ng) for r in range(ng)] if ng > 1 else [0]

    def quad_of(g):
        return lax.rem(quad + quads[g] + ng, ng)

    load(k_hbm, ks, 0)
    for g in range(ng):
        src = x_hbm.at[:, pl.ds(pl.multiple_of(quad_of(g) * (gz * blk), gz * blk), gz * blk)]
        pltpu.make_async_copy(src, xs.at[g], x_sem.at[g]).start()
    load(w_hbm, wv, 1)
    load(m_hbm, mv, 2)
    load(lr_hbm.at[0], lrv.at[c], 3)
    load(rr_hbm, rrv, 4)
    load(ls_hbm.at[0], lsv, 5)
    load(rs_hbm, rsv, 6)

    bar = pltpu.get_barrier_semaphore()
    for dx, dc in xc_peers:
        pl.semaphore_signal(bar, inc=1, device_id=xc_dev(dx, dc), device_id_type=MESH)

    @pl.loop(1, ny)
    def _(dy):
        pl.semaphore_signal(bar, inc=1, device_id={"y": ypos(dy)}, device_id_type=MESH)

    @pl.loop(1, nz)
    def _(dz):
        pl.semaphore_signal(bar, inc=1, device_id={"z": lax.rem(z + dz, nz)}, device_id_type=MESH)

    def matmul(g):
        await_bytes(xs.at[g], x_sem.at[g])
        out = jnp.dot(kt[...], xs[g], preferred_element_type=F32)
        for i in range(gz):
            for h in range(2):
                pt[g, h, i] = out[h * H:(h + 1) * H, i * blk:(i + 1) * blk]

    def exchange(g):
        send(pt.at[g, other], px.at[g], d_send.at[0], d_recv.at[g], partner)

    def span(g):
        return pl.ds(g * gz, gz)

    def scatter_y(g):
        await_bytes(px.at[g], d_recv.at[g])
        for i in range(gz):
            r = g * gz + i
            t = (pt[g, c, i] + px[g, i]).T.reshape(ny, ROWS, H)
            sf[r] = t
            ysend[:, r] = t.astype(BF16)
        for dst, via, slot in ((ypos(4), 2 * sgn, 2), (ypos(3), 1, 0), (ypos(-3), -1, 1)):
            send(ysend.at[dst, span(g)], yrel.at[slot, span(g)], ry_send.at[0], rel_recv.at[g], {"y": ypos(via)})
        for d, slot in ((1, 0), (-1, 1)):
            send(ysend.at[ypos(d), span(g)], yrecv.at[slot, span(g)], ry_send.at[1], ry_recv.at[g], {"y": ypos(d)})

    loaded(ks, 0)
    kt[...] = ks[...].T
    matmul(0)
    loaded(wv, 1)
    loaded(mv, 2)
    base = 0.9 * wv[...] - 0.225 * mv[...]
    ascr[0] = base[:, :H]
    ascr[1] = base[:, H:]
    afull[c, me, y, my8] = ascr[c]
    loaded(lrv.at[c], 3)

    pl.semaphore_wait(bar, (ny - 1) + (nz - 1) + len(xc_peers))

    exchange(0)
    send(ascr.at[other], afull.at[other, me, y, my8], d_send.at[1], d_recv.at[ng], partner)
    send(lrv.at[c], lrv.at[c], d_send.at[2], d_recv.at[ng + 1], partner)
    for g in range(1, ng):
        matmul(g)
        exchange(g)
        scatter_y(g - 1)
        if g == 1:
            await_bytes(ascr.at[0], d_recv.at[ng])

            @pl.loop(1, ny)
            def _(dy):
                send(afull.at[c, me, y], afull.at[c, me, y], a_sem.at[0], a_sem.at[1], {"y": ypos(dy)})
    scatter_y(ng - 1)
    if ng == 1:
        await_bytes(ascr.at[0], d_recv.at[ng])

        @pl.loop(1, ny)
        def _(dy):
            send(afull.at[c, me, y], afull.at[c, me, y], a_sem.at[0], a_sem.at[1], {"y": ypos(dy)})

    def ring_step(k):
        if k == 1:
            await_bytes(afull.at[c, me, pl.ds(0, ny - 1)], a_sem.at[1])
        else:
            await_bytes(afull.at[c, 0], ring_r.at[k - 2])
            if k <= half:
                await_bytes(afull.at[c, 0], ring_l.at[k - 2])
        if k <= half:
            src, dst = place_of(-(k - 1), nz), place_of(-k, nz)
            send(afull.at[c, src], afull.at[c, dst], ring_send.at[0], ring_r.at[k - 1], {"z": zpos(1)})
        if k < half:
            src, dst = place_of(k - 1, nz), place_of(k, nz)
            send(afull.at[c, src], afull.at[c, dst], ring_send.at[1], ring_l.at[k - 1], {"z": zpos(-1)})
        if k == half + 1:
            send(afull.at[c], afull.at[c], d_send.at[3], d_recv.at[ng + 2], partner)

    steps = iter(range(1, half + 2))

    def ring(n=1):
        for _ in range(n):
            k = next(steps, None)
            if k is not None:
                ring_step(k)

    up_mask = (1 - c).astype(F32)
    down_mask = c.astype(F32)
    for g in range(ng):
        await_bytes(yrel.at[:, span(g)], rel_recv.at[g])
        for i in range(gz):
            r = g * gz + i
            far = yrel[2, r].astype(F32)
            ysum[0, r] = (sf[r, ypos(2)] + yrel[0, r].astype(F32) + up_mask * far).astype(BF16)
            ysum[1, r] = (sf[r, ypos(-2)] + yrel[1, r].astype(F32) + down_mask * far).astype(BF16)
        for d, slot in ((2, 0), (-2, 1)):
            send(ysum.at[slot, span(g)], yrecv.at[2 + slot, span(g)], ry_send.at[2], ry_recv.at[g], {"y": ypos(d)})
        if g == ng // 2:
            ring()
    for g in range(ng):
        await_bytes(yrecv.at[:, span(g)], ry_recv.at[g])
        for i in range(gz):
            r = g * gz + i
            t = sf[r, y]
            for j in range(4):
                t = t + yrecv[j, r].astype(F32)
            zsend[r] = t
        for i in range(gz):
            if quads[g]:
                send(zsend.at[g * gz + i], zrecv.at[z], rz_sem.at[0], rz_sem.at[1], {"z": quad_of(g) * gz + i})
            elif i:
                at = lax.rem(zi + i, gz)
                send(zsend.at[g * gz + at], zrecv.at[z], rz_sem.at[0], rz_sem.at[1], {"z": quad * gz + at})
        if g == ng // 2:
            ring()
    zrecv[z] = zsend[(ng - 1) * gz + zi]
    ring()

    await_bytes(zrecv.at[pl.ds(0, nz - 1)], rz_sem.at[1])
    grad = zrecv[0]
    for r in range(1, nz):
        grad = grad + zrecv[r]
    sv[0:1] = jnp.sum(grad * grad, axis=0, keepdims=True)
    gfull[c, me, y] = grad.astype(BF16)

    groups = [(me, 1)] + [(r, 2) for r in range(nz - 3, 0, -2)] + [(0, 1)]
    ngr = len(groups)
    lag = min(3, ngr - 1)

    def gather_start(full, p):
        for r in range(nz - 1):
            off = offset_of(r, nz)
            back = place_of(-off, nz)
            j = [q for q, (r0, n) in enumerate(groups) if r0 <= back < r0 + n][0]
            send(full.at[c, me, y], full.at[c, back, y], ag_send.at[p, 0], agz_recv.at[p, j], {"z": zpos(off)})
        gather_forward(full, p, 0)

    def gather_forward(full, p, j):
        r0, n = groups[j]
        if j:
            await_bytes(full.at[c, pl.ds(r0, n), y], agz_recv.at[p, j])
        slab = full.at[c, pl.ds(r0, n), y]
        for d in (2, -2):
            send(slab, slab, ag_send.at[p, 1], agx_recv.at[p, j], {"y": ypos(d)})
        for d in (1, -1):
            send(slab, slab, ag_send.at[p, 1], agy_recv.at[p, j], {"y": ypos(d)})

    def gather_relay(full, p, j):
        r0, n = groups[j]
        await_bytes(full.at[c, pl.ds(r0, n), pl.ds(0, 2)], agx_recv.at[p, j])
        for origin, to in ((-2 * sgn, 2 * sgn), (-2, 1), (2, -1)):
            slab = full.at[c, pl.ds(r0, n), ypos(origin)]
            send(slab, slab, ag_send.at[p, 1], agy_recv.at[p, j], {"y": ypos(to)})

    def gather_land(full, p, j):
        r0, n = groups[j]
        await_bytes(full.at[c, pl.ds(r0, n), pl.ds(0, 5)], agy_recv.at[p, j])
        slab = full.at[c, pl.ds(r0, n)]
        send(slab, slab, ag_send.at[p, 2], agd_recv.at[p, j], partner)

    def gather(full, p, after_forward, before_land, after_land):
        for j in range(1, ngr):
            gather_forward(full, p, j)
            after_forward(j)
            if j >= lag:
                gather_relay(full, p, j - lag)
        for j in range(ngr - lag, ngr):
            gather_relay(full, p, j)
        before_land()
        for j in range(ngr):
            gather_land(full, p, j)
            after_land(j)

    def gather_close(full, p):
        await_bytes(full.at[0, pl.ds(0, nz - 1), 0], ag_send.at[p, 0])
        await_bytes(full.at[0, :, pl.ds(0, ny - 1)], ag_send.at[p, 1])
        await_bytes(full.at[0], ag_send.at[p, 2])

    def keep(h, j):
        r0, n = groups[j]
        for r in range(r0, r0 + n):
            gabs[h, pl.ds(pl.multiple_of(zpos(offset_of(r, nz)) * blk, blk), blk)] = gfull[h, r].reshape(blk, H)

    gather_start(gfull, 0)
    gather(gfull, 0, lambda j: ring() if j == ngr // 2 else None, ring, lambda j: keep(c, j))

    await_bytes(lrv.at[0], d_recv.at[ng + 1])
    loaded(rrv, 4)
    lm = jnp.concatenate([lrv[0].astype(F32), lrv[1].astype(F32)], axis=0).astype(BF16)
    left = jnp.dot(lm, gabs[c], preferred_element_type=F32)
    hi = left.astype(BF16)
    lo = (left - hi.astype(F32)).astype(BF16)
    rr = rrv[c]
    pre = jnp.dot(hi, rr, preferred_element_type=F32) + jnp.dot(lo, rr, preferred_element_type=F32)
    pfull[c, me, y] = pre.astype(BF16)
    gather_start(pfull, 1)
    sv[1:2] = jnp.sum(pre * pre, axis=0, keepdims=True)
    tile[...] = pre

    s1[x * 2 + c] = sv[...]
    for dx, dc in xc_peers:
        send(sv, s1.at[x * 2 + c], s_send.at[0], s_recv.at[0], xc_dev(dx, dc))
    send(tile.at[its8], own8.at[c], d_send.at[4], d_recv.at[ng + 3], partner)
    own8[c] = tile[my8]

    def total(buf, n):
        tot = buf[0]
        for i in range(1, n):
            tot = tot + buf[i]
        return tot

    def after_forward(j):
        if j == 1:
            await_bytes(s1.at[pl.ds(0, 2 * nx - 1)], s_recv.at[0])
            s2[z] = total(s1, 2 * nx)

            @pl.loop(1, nz)
            def _(dz):
                send(s2.at[z], s2.at[z], s_send.at[1], s_recv.at[1], {"z": lax.rem(z + dz, nz)})
        if j == ngr // 2:
            ring()

    def before_land():
        await_bytes(s2.at[pl.ds(0, nz - 1)], s_recv.at[1])
        s3[y] = total(s2, nz)

        @pl.loop(1, ny)
        def _(dy):
            send(s3.at[y], s3.at[y], s_send.at[2], s_recv.at[2], {"y": ypos(dy)})
        ring(half)

        for j in range(ngr):
            r0, n = groups[j]
            await_bytes(gfull.at[other, pl.ds(r0, n)], agd_recv.at[0, j])
            keep(other, j)
        gram = None
        for h in range(2):
            gown[...] = gfull[h, me, y].astype(F32)
            part = lax.dot_general(
                gown[my8].astype(BF16), gabs[h], (((1,), (1,)), ((), ())), preferred_element_type=F32
            )
            gram = part if gram is None else gram + part
        loaded(lsv, 5)
        lnv[...] = 0.95 * lsv[...] + 0.05 * gram
        loaded(rsv, 6)
        for h in range(2):
            gh = gabs[h]
            hg = lax.dot_general(gh, gh, (((0,), (0,)), ((), ())), preferred_element_type=F32)
            rnv[h] = 0.95 * rsv[h] + 0.05 * hg

    gather(pfull, 1, after_forward, before_land, lambda j: None)

    await_bytes(s3.at[pl.ds(0, ny - 1)], s_recv.at[2])
    tot = total(s3, ny)
    gs = jnp.sum(tot[0:1], axis=1, keepdims=True)
    ps = jnp.sum(tot[1:2], axis=1, keepdims=True)
    scale = jnp.sqrt(gs / (ps + 1e-06))

    await_bytes(own8.at[0], d_recv.at[ng + 3])
    wide = jnp.concatenate([own8[0], own8[1]], axis=1)
    mom = 0.9 * mv[...] + scale * wide
    upd = -0.25 * (mom + 0.4 * wv[...])
    momv[...] = mom
    upv[...] = upd
    wnv[...] = wv[...] + upd

    await_bytes(afull.at[other], d_recv.at[ng + 2])
    quarter = 0.25 * scale
    for j in range(ngr):
        r0, n = groups[j]
        await_bytes(pfull.at[other, pl.ds(r0, n)], agd_recv.at[1, j])
        for r in range(r0, r0 + n):
            rows = pl.ds(pl.multiple_of(zpos(offset_of(r, nz)) * blk, blk), blk)
            for h in range(2):
                v = afull[h, r].reshape(blk, H) - quarter * pfull[h, r].reshape(blk, H).astype(F32)
                outv[rows, h * H:(h + 1) * H] = v.astype(BF16)

    await_bytes(pt.at[:, 0], d_send.at[0])
    await_bytes(ascr.at[0], d_send.at[1])
    await_bytes(lrv.at[0], d_send.at[2])
    await_bytes(afull.at[0], d_send.at[3])
    await_bytes(own8.at[0], d_send.at[4])
    await_bytes(yrel, ry_send.at[0])
    await_bytes(ysum, ry_send.at[1])
    await_bytes(ysum, ry_send.at[2])
    await_bytes(zrecv.at[pl.ds(0, nz - 1)], rz_sem.at[0])
    await_bytes(afull.at[0, 0, pl.ds(0, ny - 1)], a_sem.at[0])
    await_bytes(afull.at[0, pl.ds(0, half)], ring_send.at[0])
    if half > 1:
        await_bytes(afull.at[0, pl.ds(0, half - 1)], ring_send.at[1])
    gather_close(gfull, 0)
    gather_close(pfull, 1)
    await_bytes(s1.at[pl.ds(0, 2 * nx - 1)], s_send.at[0])
    await_bytes(s2.at[pl.ds(0, nz - 1)], s_send.at[1])
    await_bytes(s3.at[pl.ds(0, ny - 1)], s_send.at[2])


def write_out(*refs):
    n = (len(refs) - 1) // 2
    sems = refs[-1]
    copies = [pltpu.make_async_copy(refs[i], refs[n + i], sems.at[i]) for i in range(n)]
    for copy in copies:
        copy.start()
    for copy in copies:
        copy.wait()


def body(nz, ny, nx, gz, inputs, key_grads, weights, momentum, left_stat, right_stat, left_root, right_root):
    tokens, width = inputs.shape
    ng, blk, ngr = nz // gz, ny * ROWS, nz // 2 + 1
    dma = pltpu.SemaphoreType.DMA
    v = pltpu.VMEM
    scratch = [
        v((ng, tokens, gz * blk), BF16), v((tokens, 2 * H), BF16), v((2 * H, tokens), BF16),
        v((ng, 2, gz, H, blk), F32), v((ng, gz, H, blk), F32),
        v((nz, ny, ROWS, H), F32), v((ny, nz, ROWS, H), BF16),
        v((3, nz, ROWS, H), BF16), v((2, nz, ROWS, H), BF16), v((4, nz, ROWS, H), BF16),
        v((nz, ROWS, H), F32), v((nz, ROWS, H), F32),
        v((2, nz, ny, ROWS, H), BF16), v((2, width, H), BF16), v((2, nz, ny, ROWS, H), BF16), v((2, nz, ny, ROWS, H), F32),
        v((2, 8, H), F32), v((ROWS, H), F32), v((2, 8, H), F32), v((ROWS, H), F32),
        v((8, 2 * H), F32), v((8, 2 * H), F32), v((8, width), F32), v((2, H, H), F32), v((2, 8, width), BF16), v((2, H, H), BF16),
        v((2, H), F32), v((2 * nx, 2, H), F32), v((nz, 2, H), F32), v((ny, 2, H), F32),
        dma((7,)), dma((ng,)), dma((5,)), dma((ng + 4,)), dma((3,)), dma((ng,)), dma((ng,)), dma((2,)), dma((2,)),
        dma((2,)), dma((nz // 2,)), dma((nz // 2,)),
        dma((2, 3)), dma((2, ngr)), dma((2, ngr)), dma((2, ngr)), dma((2, ngr)), dma((3,)), dma((3,)),
    ]
    sds = jax.ShapeDtypeStruct
    anyspace = pl.BlockSpec(memory_space=pl.ANY)
    local = pl.BlockSpec(memory_space=pltpu.VMEM)
    shapes = (
        (weights.shape, F32), ((8, width), F32), (right_stat.shape, F32),
        (weights.shape, F32), (weights.shape, F32), ((width, 2 * H), BF16),
    )
    held = pl.pallas_call(
        functools.partial(kernel, nz, ny, nx, gz),
        out_shape=tuple(HELD(*s) for s in shapes),
        in_specs=[anyspace] * 8,
        out_specs=(local,) * 6,
        scratch_shapes=scratch,
        compiler_params=pltpu.CompilerParams(collective_id=0, has_side_effects=True, vmem_limit_bytes=56 * 2**20),
    )(inputs, key_grads, weights, momentum, left_stat, right_stat, left_root, right_root)
    mom, left, right, upd, nxt, copy = pl.pallas_call(
        write_out,
        out_shape=tuple(sds(*s) for s in shapes),
        in_specs=[local] * 6,
        out_specs=(anyspace,) * 6,
        scratch_shapes=[dma((6,))],
    )(*(pltpu.with_memory_space_constraint(h, pltpu.VMEM) for h in held))
    return mom, left[None], right, upd, nxt, copy


def build(devices, nz, ny, nx, gz):
    split = Mesh(devices.reshape(nz, ny, 2, nx), ("z", "y", "c", "x"))
    fs = ("z", "y", "c")
    in_specs = (
        P(fs, None), P(fs, "x"), P(fs, "x"), P(fs, "x"),
        P("x", fs, None), P("x", None, None), P("x", fs, None), P("x", None, None),
    )
    out_specs = (P(fs, "x"), P("x", fs, None), P("x", None, None), P(fs, "x"), P(fs, "x"), P(None, "x"))
    return jax.shard_map(
        functools.partial(body, nz, ny, nx, gz), mesh=split, in_specs=in_specs, out_specs=out_specs, check_vma=False
    )


def solution(mesh):
    return build(mesh.devices, 16, 8, mesh.shape["tp"], 4)
```

```python
import functools

import jax
import jax.numpy as jnp
from jax import lax
from jax.experimental import pallas as pl
from jax.experimental.pallas import tpu as pltpu
from jax.sharding import Mesh
from jax.sharding import PartitionSpec as P

MESH = pl.DeviceIdType.MESH
F32 = jnp.float32
BF16 = jnp.bfloat16
H = 128
ROWS = 16


def offset_of(r, nz):
    half = nz // 2
    if r == 0:
        return half
    return half - (r + 1) // 2 if r % 2 else -(half - r // 2)


def place_of(off, nz):
    half = nz // 2
    if off == 0:
        return nz - 1
    if abs(off) == half:
        return 0
    return 2 * (half - off) - 1 if off > 0 else 2 * (half + off)


HELD = pltpu.VMEM


def kernel(
    nz, ny, nx, gz,
    x_hbm, k_hbm, w_hbm, m_hbm, ls_hbm, rs_hbm, lr_hbm, rr_hbm,
    momv, lnv, rnv, upv, wnv, outv,
    xs, ks, kt, pt, px, sf, ysend, yrel, ysum, yrecv, zsend, zrecv, gfull, gabs, pfull, afull, ascr, tile, own8, gown,
    wv, mv, lsv, rsv, lrv, rrv,
    sv, s1, s2, s3,
    hello, in_sem, x_sem, d_send, d_recv, ry_send, rel_recv, ry_recv, rz_sem, a_send, a_recv,
    ag_send, agz_recv, agx_recv, agy_recv, agd_recv, s_send, s_recv,
):
    ng = nz // gz
    blk = ny * ROWS
    half = nz // 2
    z, y, c, x = (lax.axis_index(n) for n in ("z", "y", "c", "x"))
    me = nz - 1
    other = 1 - c
    sgn = 1 - 2 * c
    partner = {"c": other}
    quad, zi = z // gz, lax.rem(z, gz)
    my8 = pl.ds(pl.multiple_of(8 * c, 8), 8)
    its8 = pl.ds(pl.multiple_of(8 * other, 8), 8)

    def zpos(off):
        return lax.rem(z + off + nz, nz)

    def ypos(dy):
        return lax.rem(y + dy + ny, ny)

    def send(src, dst, s, r, dev):
        pltpu.make_async_remote_copy(src, dst, s, r, device_id=dev, device_id_type=MESH).start()

    def await_bytes(ref, sem):
        pltpu.make_async_copy(ref, ref, sem).wait()

    xc_peers = [(dx, dc) for dx in range(nx) for dc in range(2) if dx or dc]

    def xc_dev(dx, dc):
        return {"x": lax.rem(x + dx, nx), "c": lax.rem(c + dc, 2)}

    def load(src, dst, i):
        pltpu.make_async_copy(src, dst, in_sem.at[i]).start()

    def loaded(dst, i):
        await_bytes(dst, in_sem.at[i])

    quads = [offset_of(r, ng) for r in range(ng)] if ng > 1 else [0]

    def quad_of(g):
        return lax.rem(quad + quads[g] + ng, ng)

    load(k_hbm, ks, 0)
    for g in range(ng):
        src = x_hbm.at[:, pl.ds(pl.multiple_of(quad_of(g) * (gz * blk), gz * blk), gz * blk)]
        pltpu.make_async_copy(src, xs.at[g], x_sem.at[g]).start()
    load(w_hbm, wv, 1)
    load(m_hbm, mv, 2)
    load(lr_hbm.at[0], lrv.at[c], 3)
    load(rr_hbm, rrv, 4)
    load(ls_hbm.at[0], lsv, 5)
    load(rs_hbm, rsv, 6)

    bar = pltpu.get_barrier_semaphore()
    for dx, dc in xc_peers:
        pl.semaphore_signal(bar, inc=1, device_id=xc_dev(dx, dc), device_id_type=MESH)

    @pl.loop(1, ny)
    def _(dy):
        pl.semaphore_signal(bar, inc=1, device_id={"y": ypos(dy)}, device_id_type=MESH)

    near = sorted({d % nz for d in range(-4, 5) if d % nz})
    for dz in near:
        pl.semaphore_signal(bar, inc=1, device_id={"z": lax.rem(z + dz, nz)}, device_id_type=MESH)

    def matmul(g):
        await_bytes(xs.at[g], x_sem.at[g])
        out = jnp.dot(kt[...], xs[g], preferred_element_type=F32)
        for i in range(gz):
            for h in range(2):
                pt[g, h, i] = out[h * H:(h + 1) * H, i * blk:(i + 1) * blk]

    def exchange(g):
        send(pt.at[g, other], px.at[g], d_send.at[0], d_recv.at[g], partner)

    def span(g):
        return pl.ds(g * gz, gz)

    def scatter_y(g):
        await_bytes(px.at[g], d_recv.at[g])
        for i in range(gz):
            r = g * gz + i
            t = (pt[g, c, i] + px[g, i]).T.reshape(ny, ROWS, H)
            sf[r] = t
            ysend[:, r] = t.astype(BF16)
        for dst, via, slot in ((ypos(4), 2 * sgn, 2), (ypos(3), 1, 0), (ypos(-3), -1, 1)):
            send(ysend.at[dst, span(g)], yrel.at[slot, span(g)], ry_send.at[0], rel_recv.at[g], {"y": ypos(via)})
        for d, slot in ((1, 0), (-1, 1)):
            send(ysend.at[ypos(d), span(g)], yrecv.at[slot, span(g)], ry_send.at[1], ry_recv.at[g], {"y": ypos(d)})

    loaded(ks, 0)
    kt[...] = ks[...].T
    matmul(0)
    loaded(wv, 1)
    loaded(mv, 2)
    base = 0.9 * wv[...] - 0.225 * mv[...]
    ascr[0] = base[:, :H]
    ascr[1] = base[:, H:]
    afull[c, me, y, my8] = ascr[c]
    loaded(lrv.at[c], 3)

    pl.semaphore_wait(bar, (ny - 1) + len(near) + len(xc_peers))
    far = len(near) < nz - 1
    if far:
        for dz in (4, -4):
            pl.semaphore_signal(hello, inc=1, device_id={"z": zpos(dz)}, device_id_type=MESH)

    exchange(0)
    send(ascr.at[other], afull.at[other, me, y, my8], d_send.at[1], d_recv.at[ng], partner)
    send(lrv.at[c], lrv.at[c], d_send.at[2], d_recv.at[ng + 1], partner)
    up_mask = (1 - c).astype(F32)
    down_mask = c.astype(F32)

    def relay_y(g):
        await_bytes(yrel.at[:, span(g)], rel_recv.at[g])
        for i in range(gz):
            r = g * gz + i
            far = yrel[2, r].astype(F32)
            ysum[0, r] = (sf[r, ypos(2)] + yrel[0, r].astype(F32) + up_mask * far).astype(BF16)
            ysum[1, r] = (sf[r, ypos(-2)] + yrel[1, r].astype(F32) + down_mask * far).astype(BF16)
        for d, slot in ((2, 0), (-2, 1)):
            send(ysum.at[slot, span(g)], yrecv.at[2 + slot, span(g)], ry_send.at[2], ry_recv.at[g], {"y": ypos(d)})

    def scatter_z(g):
        await_bytes(yrecv.at[:, span(g)], ry_recv.at[g])
        for i in range(gz):
            r = g * gz + i
            t = sf[r, y]
            for j in range(4):
                t = t + yrecv[j, r].astype(F32)
            zsend[r] = t
        for i in range(gz):
            if quads[g]:
                send(zsend.at[g * gz + i], zrecv.at[z], rz_sem.at[0], rz_sem.at[1], {"z": quad_of(g) * gz + i})
            elif i:
                at = lax.rem(zi + i, gz)
                send(zsend.at[g * gz + at], zrecv.at[z], rz_sem.at[0], rz_sem.at[1], {"z": quad * gz + at})

    pieces = ((0, half), (half, nz - half))

    def base_z(is_near):
        if is_near:
            await_bytes(ascr.at[0], d_recv.at[ng])
        elif far:
            pl.semaphore_wait(hello, 2)
        for r in range(nz - 1):
            off = offset_of(r, nz)
            if (off % nz in near) != is_near:
                continue
            send(afull.at[c, me, y], afull.at[c, place_of(-off, nz), y], a_send.at[0], a_recv.at[0], {"z": zpos(off)})

    def base_y(p):
        r0, n = pieces[p]
        if p == 0:
            await_bytes(afull.at[c, pl.ds(0, nz - 1), y], a_recv.at[0])
        slab = afull.at[c, pl.ds(r0, n), y]
        for d in (2, -2):
            send(slab, slab, a_send.at[1], a_recv.at[1 + p], {"y": ypos(d)})
        for d in (1, -1):
            send(slab, slab, a_send.at[1], a_recv.at[3 + p], {"y": ypos(d)})

    def base_relay(p):
        r0, n = pieces[p]
        await_bytes(afull.at[c, pl.ds(r0, n), pl.ds(0, 2)], a_recv.at[1 + p])
        for origin, to in ((-2 * sgn, 2 * sgn), (-2, 1), (2, -1)):
            slab = afull.at[c, pl.ds(r0, n), ypos(origin)]
            send(slab, slab, a_send.at[1], a_recv.at[3 + p], {"y": ypos(to)})

    def base_land(p):
        r0, n = pieces[p]
        await_bytes(afull.at[c, pl.ds(r0, n), pl.ds(0, 5)], a_recv.at[3 + p])
        slab = afull.at[c, pl.ds(r0, n)]
        send(slab, slab, d_send.at[3], a_recv.at[5 + p], partner)

    for g in range(1, ng):
        matmul(g)
        exchange(g)
        scatter_y(g - 1)
        if g == 1:
            base_z(True)
    if ng == 1:
        base_z(True)
    base_z(False)
    early = min(2, ng - 1)
    if early:
        relay_y(0)
    scatter_y(ng - 1)
    for g in range(1 if early else 0, ng - 1):
        relay_y(g)
    if ng > 1:
        scatter_z(0)
    relay_y(ng - 1)
    for g in range(1 if ng > 1 else 0, ng):
        scatter_z(g)
    zrecv[z] = zsend[(ng - 1) * gz + zi]
    base_y(0)
    base_y(1)

    await_bytes(zrecv.at[pl.ds(0, nz - 1)], rz_sem.at[1])
    grad = zrecv[0]
    for r in range(1, nz):
        grad = grad + zrecv[r]
    sv[0:1] = jnp.sum(grad * grad, axis=0, keepdims=True)
    gfull[c, me, y] = grad.astype(BF16)

    groups = [(me, 1)] + [(r, 2) for r in range(nz - 3, 0, -2)] + [(0, 1)]
    ngr = len(groups)
    lag = min(5, ngr - 1)
    direct = range(max(ngr - 2, 1), ngr)

    def gather_start(full, p):
        order = [0, 1, 2, 13, 14, 3, 4, 11, 12, 5, 6, 9, 10, 7, 8] if nz == 16 else range(nz - 1)
        for r in order:
            off = offset_of(r, nz)
            back = place_of(-off, nz)
            j = [q for q, (r0, n) in enumerate(groups) if r0 <= back < r0 + n][0]
            send(full.at[c, me, y], full.at[c, back, y], ag_send.at[p, 0], agz_recv.at[p, j], {"z": zpos(off)})
        gather_forward(full, p, 0)

    def gather_forward(full, p, j):
        r0, n = groups[j]
        if j:
            await_bytes(full.at[c, pl.ds(r0, n), y], agz_recv.at[p, j])
        slab = full.at[c, pl.ds(r0, n), y]
        if j in direct:
            for d in (4, 3, -3, 2, -2, 1, -1):
                send(slab, slab, ag_send.at[p, 1], agy_recv.at[p, j], {"y": ypos(d)})
            return
        for d in (2, -2):
            send(slab, slab, ag_send.at[p, 1], agx_recv.at[p, j], {"y": ypos(d)})
        for d in (1, -1):
            send(slab, slab, ag_send.at[p, 1], agy_recv.at[p, j], {"y": ypos(d)})

    def gather_relay(full, p, j):
        if j in direct:
            return
        r0, n = groups[j]
        await_bytes(full.at[c, pl.ds(r0, n), pl.ds(0, 2)], agx_recv.at[p, j])
        for origin, to in ((-2 * sgn, 2 * sgn), (-2, 1), (2, -1)):
            slab = full.at[c, pl.ds(r0, n), ypos(origin)]
            send(slab, slab, ag_send.at[p, 1], agy_recv.at[p, j], {"y": ypos(to)})

    def gather_land(full, p, j):
        r0, n = groups[j]
        await_bytes(full.at[c, pl.ds(r0, n), pl.ds(0, ny - 1 if j in direct else 5)], agy_recv.at[p, j])
        slab = full.at[c, pl.ds(r0, n)]
        send(slab, slab, ag_send.at[p, 2], agd_recv.at[p, j], partner)

    def gather(full, p, after_forward, before_land, after_land):
        for j in range(1, ngr):
            gather_forward(full, p, j)
            after_forward(j)
            if j >= lag:
                gather_relay(full, p, j - lag)
        for j in range(ngr - lag, ngr):
            gather_relay(full, p, j)
        before_land()
        for j in range(ngr):
            gather_land(full, p, j)
            after_land(j)

    def gather_close(full, p):
        await_bytes(full.at[0, pl.ds(0, nz - 1), 0], ag_send.at[p, 0])
        await_bytes(full.at[0, :, pl.ds(0, ny - 1)], ag_send.at[p, 1])
        await_bytes(full.at[0], ag_send.at[p, 2])

    def keep(h, j):
        r0, n = groups[j]
        for r in range(r0, r0 + n):
            gabs[h, pl.ds(pl.multiple_of(zpos(offset_of(r, nz)) * blk, blk), blk)] = gfull[h, r].reshape(blk, H)

    gather_start(gfull, 0)
    gather(gfull, 0, lambda j: None, lambda: None, lambda j: keep(c, j))

    await_bytes(lrv.at[0], d_recv.at[ng + 1])
    loaded(rrv, 4)
    lm = jnp.concatenate([lrv[0].astype(F32), lrv[1].astype(F32)], axis=0).astype(BF16)
    left = jnp.dot(lm, gabs[c], preferred_element_type=F32)
    hi = left.astype(BF16)
    lo = (left - hi.astype(F32)).astype(BF16)
    rr = rrv[c]
    pre = jnp.dot(hi, rr, preferred_element_type=F32) + jnp.dot(lo, rr, preferred_element_type=F32)
    pfull[c, me, y] = pre.astype(BF16)
    gather_start(pfull, 1)
    for p in range(2):
        base_relay(p)
    sv[1:2] = jnp.sum(pre * pre, axis=0, keepdims=True)
    tile[...] = pre

    s2[z] = sv[...]

    @pl.loop(1, nz)
    def _(dz):
        send(sv, s2.at[z], s_send.at[1], s_recv.at[1], {"z": lax.rem(z + dz, nz)})

    send(tile.at[its8], own8.at[c], d_send.at[4], d_recv.at[ng + 3], partner)
    own8[c] = tile[my8]

    def total(buf, n):
        tot = buf[0]
        for i in range(1, n):
            tot = tot + buf[i]
        return tot

    def after_forward(j):
        if j == ngr - 1:
            await_bytes(s2.at[pl.ds(0, nz - 1)], s_recv.at[1])
            s3[y] = total(s2, nz)

            @pl.loop(1, ny)
            def _(dy):
                send(s3.at[y], s3.at[y], s_send.at[2], s_recv.at[2], {"y": ypos(dy)})

    def before_land():
        for j in range(ngr):
            r0, n = groups[j]
            await_bytes(gfull.at[other, pl.ds(r0, n)], agd_recv.at[0, j])
            keep(other, j)
        gram = None
        for h in range(2):
            gown[...] = gfull[h, me, y].astype(F32)
            part = lax.dot_general(
                gown[my8].astype(BF16), gabs[h], (((1,), (1,)), ((), ())), preferred_element_type=F32
            )
            gram = part if gram is None else gram + part
        loaded(lsv, 5)
        lnv[...] = 0.95 * lsv[...] + 0.05 * gram
        loaded(rsv, 6)
        for h in range(2):
            gh = gabs[h]
            hg = lax.dot_general(gh, gh, (((0,), (0,)), ((), ())), preferred_element_type=F32)
            rnv[h] = 0.95 * rsv[h] + 0.05 * hg
        for p in range(2):
            base_land(p)
        await_bytes(s3.at[pl.ds(0, ny - 1)], s_recv.at[2])
        s1[x * 2 + c] = total(s3, ny)
        for dx, dc in xc_peers:
            send(s1.at[x * 2 + c], s1.at[x * 2 + c], s_send.at[0], s_recv.at[0], xc_dev(dx, dc))

    gather(pfull, 1, after_forward, before_land, lambda j: None)

    await_bytes(s1.at[pl.ds(0, 2 * nx - 1)], s_recv.at[0])
    tot = total(s1, 2 * nx)
    gs = jnp.sum(tot[0:1], axis=1, keepdims=True)
    ps = jnp.sum(tot[1:2], axis=1, keepdims=True)
    scale = jnp.sqrt(gs / (ps + 1e-06))

    await_bytes(own8.at[0], d_recv.at[ng + 3])
    wide = jnp.concatenate([own8[0], own8[1]], axis=1)
    mom = 0.9 * mv[...] + scale * wide
    upd = -0.25 * (mom + 0.4 * wv[...])
    momv[...] = mom
    upv[...] = upd
    wnv[...] = wv[...] + upd

    for p in range(2):
        await_bytes(afull.at[other, pl.ds(*pieces[p])], a_recv.at[5 + p])
    quarter = 0.25 * scale
    for j in range(ngr):
        r0, n = groups[j]
        await_bytes(pfull.at[other, pl.ds(r0, n)], agd_recv.at[1, j])
        for r in range(r0, r0 + n):
            rows = pl.ds(pl.multiple_of(zpos(offset_of(r, nz)) * blk, blk), blk)
            for h in range(2):
                v = afull[h, r].reshape(blk, H) - quarter * pfull[h, r].reshape(blk, H).astype(F32)
                outv[rows, h * H:(h + 1) * H] = v.astype(BF16)

    await_bytes(pt.at[:, 0], d_send.at[0])
    await_bytes(ascr.at[0], d_send.at[1])
    await_bytes(lrv.at[0], d_send.at[2])
    await_bytes(afull.at[0], d_send.at[3])
    await_bytes(own8.at[0], d_send.at[4])
    await_bytes(yrel, ry_send.at[0])
    await_bytes(ysum, ry_send.at[1])
    await_bytes(ysum, ry_send.at[2])
    await_bytes(zrecv.at[pl.ds(0, nz - 1)], rz_sem.at[0])
    await_bytes(afull.at[0, pl.ds(0, nz - 1), 0], a_send.at[0])
    await_bytes(afull.at[0, :, pl.ds(0, ny - 1)], a_send.at[1])
    gather_close(gfull, 0)
    gather_close(pfull, 1)
    await_bytes(s1.at[pl.ds(0, 2 * nx - 1)], s_send.at[0])
    await_bytes(s2.at[pl.ds(0, nz - 1)], s_send.at[1])
    await_bytes(s3.at[pl.ds(0, ny - 1)], s_send.at[2])


def write_out(*refs):
    n = (len(refs) - 1) // 2
    sems = refs[-1]
    copies = [pltpu.make_async_copy(refs[i], refs[n + i], sems.at[i]) for i in range(n)]
    for copy in copies:
        copy.start()
    for copy in copies:
        copy.wait()


def body(nz, ny, nx, gz, inputs, key_grads, weights, momentum, left_stat, right_stat, left_root, right_root):
    tokens, width = inputs.shape
    ng, blk, ngr = nz // gz, ny * ROWS, nz // 2 + 1
    dma = pltpu.SemaphoreType.DMA
    v = pltpu.VMEM
    scratch = [
        v((ng, tokens, gz * blk), BF16), v((tokens, 2 * H), BF16), v((2 * H, tokens), BF16),
        v((ng, 2, gz, H, blk), F32), v((ng, gz, H, blk), F32),
        v((nz, ny, ROWS, H), F32), v((ny, nz, ROWS, H), BF16),
        v((3, nz, ROWS, H), BF16), v((2, nz, ROWS, H), BF16), v((4, nz, ROWS, H), BF16),
        v((nz, ROWS, H), F32), v((nz, ROWS, H), F32),
        v((2, nz, ny, ROWS, H), BF16), v((2, width, H), BF16), v((2, nz, ny, ROWS, H), BF16), v((2, nz, ny, ROWS, H), F32),
        v((2, 8, H), F32), v((ROWS, H), F32), v((2, 8, H), F32), v((ROWS, H), F32),
        v((8, 2 * H), F32), v((8, 2 * H), F32), v((8, width), F32), v((2, H, H), F32), v((2, 8, width), BF16), v((2, H, H), BF16),
        v((2, H), F32), v((2 * nx, 2, H), F32), v((nz, 2, H), F32), v((ny, 2, H), F32),
        pltpu.SemaphoreType.REGULAR, dma((7,)), dma((ng,)), dma((5,)), dma((ng + 4,)), dma((3,)), dma((ng,)), dma((ng,)), dma((2,)), dma((2,)), dma((7,)),
        dma((2, 3)), dma((2, ngr)), dma((2, ngr)), dma((2, ngr)), dma((2, ngr)), dma((3,)), dma((3,)),
    ]
    sds = jax.ShapeDtypeStruct
    anyspace = pl.BlockSpec(memory_space=pl.ANY)
    local = pl.BlockSpec(memory_space=pltpu.VMEM)
    shapes = (
        (weights.shape, F32), ((8, width), F32), (right_stat.shape, F32),
        (weights.shape, F32), (weights.shape, F32), ((width, 2 * H), BF16),
    )
    held = pl.pallas_call(
        functools.partial(kernel, nz, ny, nx, gz),
        out_shape=tuple(HELD(*s) for s in shapes),
        in_specs=[anyspace] * 8,
        out_specs=(local,) * 6,
        scratch_shapes=scratch,
        compiler_params=pltpu.CompilerParams(collective_id=0, has_side_effects=True, vmem_limit_bytes=56 * 2**20),
    )(inputs, key_grads, weights, momentum, left_stat, right_stat, left_root, right_root)
    mom, left, right, upd, nxt, copy = pl.pallas_call(
        write_out,
        out_shape=tuple(sds(*s) for s in shapes),
        in_specs=[local] * 6,
        out_specs=(anyspace,) * 6,
        scratch_shapes=[dma((6,))],
    )(*(pltpu.with_memory_space_constraint(h, pltpu.VMEM) for h in held))
    return mom, left[None], right, upd, nxt, copy


def build(devices, nz, ny, nx, gz):
    split = Mesh(devices.reshape(nz, ny, 2, nx), ("z", "y", "c", "x"))
    fs = ("z", "y", "c")
    in_specs = (
        P(fs, None), P(fs, "x"), P(fs, "x"), P(fs, "x"),
        P("x", fs, None), P("x", None, None), P("x", fs, None), P("x", None, None),
    )
    out_specs = (P(fs, "x"), P("x", fs, None), P("x", None, None), P(fs, "x"), P(fs, "x"), P(None, "x"))
    return jax.shard_map(
        functools.partial(body, nz, ny, nx, gz), mesh=split, in_specs=in_specs, out_specs=out_specs, check_vma=False
    )


def solution(mesh):
    return build(mesh.devices, 16, 8, mesh.shape["tp"], 4)
```

```python
import functools

import jax
import jax.numpy as jnp
from jax import lax
from jax.experimental import pallas as pl
from jax.experimental.pallas import tpu as pltpu
from jax.sharding import Mesh
from jax.sharding import PartitionSpec as P

MESH = pl.DeviceIdType.MESH
F32 = jnp.float32
BF16 = jnp.bfloat16
H = 128
ROWS = 16


def offset_of(r, nz):
    half = nz // 2
    if r == 0:
        return half
    return half - (r + 1) // 2 if r % 2 else -(half - r // 2)


def place_of(off, nz):
    half = nz // 2
    if off == 0:
        return nz - 1
    if abs(off) == half:
        return 0
    return 2 * (half - off) - 1 if off > 0 else 2 * (half + off)


HELD = pltpu.VMEM


def kernel(
    nz, ny, nx, gz,
    x_hbm, k_hbm, w_hbm, m_hbm, ls_hbm, rs_hbm, lr_hbm, rr_hbm,
    momv, lnv, rnv, upv, wnv, outv,
    xs, ks, kt, pt, px, sf, ysend, yrel, ysum, yrecv, zsend, zrecv, gfull, gabs, pfull, afull, ascr, tile, own8, gown,
    wv, mv, lsv, rsv, lrv, rrv,
    sv, s1, s2, s3,
    hello, in_sem, x_sem, d_send, d_recv, ry_send, rel_recv, ry_recv, rz_sem, a_send, a_recv,
    ag_send, agz_recv, agx_recv, agy_recv, agd_recv, s_send, s_recv,
):
    ng = nz // gz
    blk = ny * ROWS
    half = nz // 2
    z, y, c, x = (lax.axis_index(n) for n in ("z", "y", "c", "x"))
    me = nz - 1
    other = 1 - c
    sgn = 1 - 2 * c
    partner = {"c": other}
    quad, zi = z // gz, lax.rem(z, gz)
    my8 = pl.ds(pl.multiple_of(8 * c, 8), 8)
    its8 = pl.ds(pl.multiple_of(8 * other, 8), 8)

    def zpos(off):
        return lax.rem(z + off + nz, nz)

    def ypos(dy):
        return lax.rem(y + dy + ny, ny)

    def send(src, dst, s, r, dev):
        pltpu.make_async_remote_copy(src, dst, s, r, device_id=dev, device_id_type=MESH).start()

    def await_bytes(ref, sem):
        pltpu.make_async_copy(ref, ref, sem).wait()

    xc_peers = [(dx, dc) for dx in range(nx) for dc in range(2) if dx or dc]

    def xc_dev(dx, dc):
        return {"x": lax.rem(x + dx, nx), "c": lax.rem(c + dc, 2)}

    def load(src, dst, i):
        pltpu.make_async_copy(src, dst, in_sem.at[i]).start()

    def loaded(dst, i):
        await_bytes(dst, in_sem.at[i])

    quads = [offset_of(r, ng) for r in range(ng)] if ng > 1 else [0]

    def quad_of(g):
        return lax.rem(quad + quads[g] + ng, ng)

    load(k_hbm, ks, 0)
    for g in range(ng):
        src = x_hbm.at[:, pl.ds(pl.multiple_of(quad_of(g) * (gz * blk), gz * blk), gz * blk)]
        pltpu.make_async_copy(src, xs.at[g], x_sem.at[g]).start()
    load(w_hbm, wv, 1)
    load(m_hbm, mv, 2)
    load(lr_hbm.at[0], lrv.at[c], 3)
    load(rr_hbm, rrv, 4)
    load(ls_hbm.at[0], lsv, 5)
    load(rs_hbm, rsv, 6)

    bar = pltpu.get_barrier_semaphore()
    for dx, dc in xc_peers:
        pl.semaphore_signal(bar, inc=1, device_id=xc_dev(dx, dc), device_id_type=MESH)

    @pl.loop(1, ny)
    def _(dy):
        pl.semaphore_signal(bar, inc=1, device_id={"y": ypos(dy)}, device_id_type=MESH)

    near = sorted({d % nz for d in range(-4, 5) if d % nz})
    for dz in near:
        pl.semaphore_signal(bar, inc=1, device_id={"z": lax.rem(z + dz, nz)}, device_id_type=MESH)

    def matmul(g):
        await_bytes(xs.at[g], x_sem.at[g])
        out = jnp.dot(kt[...], xs[g], preferred_element_type=F32)
        for i in range(gz):
            for h in range(2):
                pt[g, h, i] = out[h * H:(h + 1) * H, i * blk:(i + 1) * blk]

    def exchange(g):
        send(pt.at[g, other], px.at[g], d_send.at[0], d_recv.at[g], partner)

    def span(g):
        return pl.ds(g * gz, gz)

    def scatter_y(g):
        await_bytes(px.at[g], d_recv.at[g])
        for i in range(gz):
            r = g * gz + i
            t = (pt[g, c, i] + px[g, i]).T.reshape(ny, ROWS, H)
            sf[r] = t
            ysend[:, r] = t.astype(BF16)
        for dst, via, slot in ((ypos(4), 2 * sgn, 2), (ypos(3), 1, 0), (ypos(-3), -1, 1)):
            send(ysend.at[dst, span(g)], yrel.at[slot, span(g)], ry_send.at[0], rel_recv.at[g], {"y": ypos(via)})
        for d, slot in ((1, 0), (-1, 1)):
            send(ysend.at[ypos(d), span(g)], yrecv.at[slot, span(g)], ry_send.at[1], ry_recv.at[g], {"y": ypos(d)})

    loaded(ks, 0)
    kt[...] = ks[...].T
    matmul(0)
    loaded(wv, 1)
    loaded(mv, 2)
    base = 0.9 * wv[...] - 0.225 * mv[...]
    ascr[0] = base[:, :H]
    ascr[1] = base[:, H:]
    afull[c, me, y, my8] = ascr[c]
    loaded(lrv.at[c], 3)

    pl.semaphore_wait(bar, (ny - 1) + len(near) + len(xc_peers))
    far = len(near) < nz - 1
    if far:
        for dz in (4, -4):
            pl.semaphore_signal(hello, inc=1, device_id={"z": zpos(dz)}, device_id_type=MESH)

    exchange(0)
    send(ascr.at[other], afull.at[other, me, y, my8], d_send.at[1], d_recv.at[ng], partner)
    send(lrv.at[c], lrv.at[c], d_send.at[2], d_recv.at[ng + 1], partner)
    up_mask = (1 - c).astype(F32)
    down_mask = c.astype(F32)

    def relay_y(g):
        await_bytes(yrel.at[:, span(g)], rel_recv.at[g])
        for i in range(gz):
            r = g * gz + i
            far = yrel[2, r].astype(F32)
            ysum[0, r] = (sf[r, ypos(2)] + yrel[0, r].astype(F32) + up_mask * far).astype(BF16)
            ysum[1, r] = (sf[r, ypos(-2)] + yrel[1, r].astype(F32) + down_mask * far).astype(BF16)
        for d, slot in ((2, 0), (-2, 1)):
            send(ysum.at[slot, span(g)], yrecv.at[2 + slot, span(g)], ry_send.at[2], ry_recv.at[g], {"y": ypos(d)})

    def scatter_z(g):
        await_bytes(yrecv.at[:, span(g)], ry_recv.at[g])
        for i in range(gz):
            r = g * gz + i
            t = sf[r, y]
            for j in range(4):
                t = t + yrecv[j, r].astype(F32)
            zsend[r] = t
        for i in range(gz):
            if quads[g]:
                send(zsend.at[g * gz + i], zrecv.at[z], rz_sem.at[0], rz_sem.at[1], {"z": quad_of(g) * gz + i})
            elif i:
                at = lax.rem(zi + i, gz)
                send(zsend.at[g * gz + at], zrecv.at[z], rz_sem.at[0], rz_sem.at[1], {"z": quad * gz + at})

    pieces = ((0, half), (half, nz - half))

    def base_z(is_near):
        if is_near:
            await_bytes(ascr.at[0], d_recv.at[ng])
        elif far:
            pl.semaphore_wait(hello, 2)
        for r in range(nz - 1):
            off = offset_of(r, nz)
            if (off % nz in near) != is_near:
                continue
            send(afull.at[c, me, y], afull.at[c, place_of(-off, nz), y], a_send.at[0], a_recv.at[0], {"z": zpos(off)})

    def base_y(p):
        r0, n = pieces[p]
        if p == 0:
            await_bytes(afull.at[c, pl.ds(0, nz - 1), y], a_recv.at[0])
        slab = afull.at[c, pl.ds(r0, n), y]
        for d in (2, -2):
            send(slab, slab, a_send.at[1], a_recv.at[1 + p], {"y": ypos(d)})
        for d in (1, -1):
            send(slab, slab, a_send.at[1], a_recv.at[3 + p], {"y": ypos(d)})

    def base_relay(p):
        r0, n = pieces[p]
        await_bytes(afull.at[c, pl.ds(r0, n), pl.ds(0, 2)], a_recv.at[1 + p])
        for origin, to in ((-2 * sgn, 2 * sgn), (-2, 1), (2, -1)):
            slab = afull.at[c, pl.ds(r0, n), ypos(origin)]
            send(slab, slab, a_send.at[1], a_recv.at[3 + p], {"y": ypos(to)})

    def base_land(p):
        r0, n = pieces[p]
        await_bytes(afull.at[c, pl.ds(r0, n), pl.ds(0, 5)], a_recv.at[3 + p])
        slab = afull.at[c, pl.ds(r0, n)]
        send(slab, slab, d_send.at[3], a_recv.at[5 + p], partner)

    for g in range(1, ng):
        matmul(g)
        exchange(g)
        scatter_y(g - 1)
        if g == 1:
            base_z(True)
    if ng == 1:
        base_z(True)
    base_z(False)
    early = min(2, ng - 1)
    if early:
        relay_y(0)
    scatter_y(ng - 1)
    for g in range(1 if early else 0, ng - 1):
        relay_y(g)
    if ng > 1:
        scatter_z(0)
    relay_y(ng - 1)
    for g in range(1 if ng > 1 else 0, ng):
        scatter_z(g)
    zrecv[z] = zsend[(ng - 1) * gz + zi]
    base_y(0)
    base_y(1)

    await_bytes(zrecv.at[pl.ds(0, nz - 1)], rz_sem.at[1])
    grad = zrecv[0]
    for r in range(1, nz):
        grad = grad + zrecv[r]
    sv[0:1] = jnp.sum(grad * grad, axis=0, keepdims=True)
    gfull[c, me, y] = grad.astype(BF16)

    groups = [(me, 1), (13, 2), (9, 4), (5, 4), (1, 4), (0, 1)] if nz == 16 else [(me, 1)] + [(r, 2) for r in range(nz - 3, 0, -2)] + [(0, 1)]
    ngr = len(groups)
    lag = min(3, ngr - 1)
    direct = range(max(ngr - 2, 1), ngr)

    def gather_start(full, p):
        order = [*range(nz - 3, nz - 1), *range(nz - 3)] if nz > 2 else [0]
        for r in order:
            off = offset_of(r, nz)
            back = place_of(-off, nz)
            j = [q for q, (r0, n) in enumerate(groups) if r0 <= back < r0 + n][0]
            send(full.at[c, me, y], full.at[c, back, y], ag_send.at[p, 0], agz_recv.at[p, j], {"z": zpos(off)})
        gather_forward(full, p, 0)

    def gather_forward(full, p, j):
        r0, n = groups[j]
        if j:
            await_bytes(full.at[c, pl.ds(r0, n), y], agz_recv.at[p, j])
        slab = full.at[c, pl.ds(r0, n), y]
        if j in direct:
            for d in (4, 3, -3, 2, -2, 1, -1):
                send(slab, slab, ag_send.at[p, 1], agy_recv.at[p, j], {"y": ypos(d)})
            return
        for d in (2, -2):
            send(slab, slab, ag_send.at[p, 1], agx_recv.at[p, j], {"y": ypos(d)})
        for d in (1, -1):
            send(slab, slab, ag_send.at[p, 1], agy_recv.at[p, j], {"y": ypos(d)})

    def gather_relay(full, p, j):
        if j in direct:
            return
        r0, n = groups[j]
        await_bytes(full.at[c, pl.ds(r0, n), pl.ds(0, 2)], agx_recv.at[p, j])
        for origin, to in ((-2 * sgn, 2 * sgn), (-2, 1), (2, -1)):
            slab = full.at[c, pl.ds(r0, n), ypos(origin)]
            send(slab, slab, ag_send.at[p, 1], agy_recv.at[p, j], {"y": ypos(to)})

    def gather_land(full, p, j):
        r0, n = groups[j]
        await_bytes(full.at[c, pl.ds(r0, n), pl.ds(0, ny - 1 if j in direct else 5)], agy_recv.at[p, j])
        slab = full.at[c, pl.ds(r0, n)]
        send(slab, slab, ag_send.at[p, 2], agd_recv.at[p, j], partner)

    def gather(full, p, after_forward, before_land, after_land):
        for j in range(1, ngr):
            gather_forward(full, p, j)
            after_forward(j)
            if j >= lag:
                gather_relay(full, p, j - lag)
        for j in range(ngr - lag, ngr):
            gather_relay(full, p, j)
        before_land()
        for j in range(ngr):
            gather_land(full, p, j)
            after_land(j)

    def gather_close(full, p):
        await_bytes(full.at[0, pl.ds(0, nz - 1), 0], ag_send.at[p, 0])
        await_bytes(full.at[0, :, pl.ds(0, ny - 1)], ag_send.at[p, 1])
        await_bytes(full.at[0], ag_send.at[p, 2])

    def keep(h, j):
        r0, n = groups[j]
        for r in range(r0, r0 + n):
            gabs[h, pl.ds(pl.multiple_of(zpos(offset_of(r, nz)) * blk, blk), blk)] = gfull[h, r].reshape(blk, H)

    gather_start(gfull, 0)
    gather(gfull, 0, lambda j: None, lambda: None, lambda j: keep(c, j))

    await_bytes(lrv.at[0], d_recv.at[ng + 1])
    loaded(rrv, 4)
    lm = jnp.concatenate([lrv[0].astype(F32), lrv[1].astype(F32)], axis=0).astype(BF16)
    left = jnp.dot(lm, gabs[c], preferred_element_type=F32)
    hi = left.astype(BF16)
    lo = (left - hi.astype(F32)).astype(BF16)
    rr = rrv[c]
    pre = jnp.dot(hi, rr, preferred_element_type=F32) + jnp.dot(lo, rr, preferred_element_type=F32)
    pfull[c, me, y] = pre.astype(BF16)
    gather_start(pfull, 1)
    sv[1:2] = jnp.sum(pre * pre, axis=0, keepdims=True)
    tile[...] = pre

    s3[y] = sv[...]

    @pl.loop(1, ny)
    def _(dy):
        send(sv, s3.at[y], s_send.at[2], s_recv.at[2], {"y": ypos(dy)})

    for p in range(2):
        base_relay(p)
    send(tile.at[its8], own8.at[c], d_send.at[4], d_recv.at[ng + 3], partner)
    own8[c] = tile[my8]

    def total(buf, n):
        tot = buf[0]
        for i in range(1, n):
            tot = tot + buf[i]
        return tot

    await_bytes(s3.at[pl.ds(0, ny - 1)], s_recv.at[2])
    s2[z] = total(s3, ny)

    @pl.loop(1, nz)
    def _(dz):
        send(s2.at[z], s2.at[z], s_send.at[1], s_recv.at[1], {"z": lax.rem(z + dz, nz)})

    def before_land():
        for j in range(ngr):
            r0, n = groups[j]
            await_bytes(gfull.at[other, pl.ds(r0, n)], agd_recv.at[0, j])
            keep(other, j)
        gram = None
        for h in range(2):
            gown[...] = gfull[h, me, y].astype(F32)
            part = lax.dot_general(
                gown[my8].astype(BF16), gabs[h], (((1,), (1,)), ((), ())), preferred_element_type=F32
            )
            gram = part if gram is None else gram + part
        loaded(lsv, 5)
        lnv[...] = 0.95 * lsv[...] + 0.05 * gram
        loaded(rsv, 6)
        for h in range(2):
            gh = gabs[h]
            hg = lax.dot_general(gh, gh, (((0,), (0,)), ((), ())), preferred_element_type=F32)
            rnv[h] = 0.95 * rsv[h] + 0.05 * hg
        for p in range(2):
            base_land(p)
        await_bytes(s2.at[pl.ds(0, nz - 1)], s_recv.at[1])
        s1[x * 2 + c] = total(s2, nz)
        for dx, dc in xc_peers:
            send(s1.at[x * 2 + c], s1.at[x * 2 + c], s_send.at[0], s_recv.at[0], xc_dev(dx, dc))

    gather(pfull, 1, lambda j: None, before_land, lambda j: None)

    await_bytes(s1.at[pl.ds(0, 2 * nx - 1)], s_recv.at[0])
    tot = total(s1, 2 * nx)
    gs = jnp.sum(tot[0:1], axis=1, keepdims=True)
    ps = jnp.sum(tot[1:2], axis=1, keepdims=True)
    scale = jnp.sqrt(gs / (ps + 1e-06))

    await_bytes(own8.at[0], d_recv.at[ng + 3])
    wide = jnp.concatenate([own8[0], own8[1]], axis=1)
    mom = 0.9 * mv[...] + scale * wide
    upd = -0.25 * (mom + 0.4 * wv[...])
    momv[...] = mom
    upv[...] = upd
    wnv[...] = wv[...] + upd

    for p in range(2):
        await_bytes(afull.at[other, pl.ds(*pieces[p])], a_recv.at[5 + p])
    quarter = 0.25 * scale
    for j in range(ngr):
        r0, n = groups[j]
        await_bytes(pfull.at[other, pl.ds(r0, n)], agd_recv.at[1, j])
        for r in range(r0, r0 + n):
            rows = pl.ds(pl.multiple_of(zpos(offset_of(r, nz)) * blk, blk), blk)
            for h in range(2):
                v = afull[h, r].reshape(blk, H) - quarter * pfull[h, r].reshape(blk, H).astype(F32)
                outv[rows, h * H:(h + 1) * H] = v.astype(BF16)

    await_bytes(pt.at[:, 0], d_send.at[0])
    await_bytes(ascr.at[0], d_send.at[1])
    await_bytes(lrv.at[0], d_send.at[2])
    await_bytes(afull.at[0], d_send.at[3])
    await_bytes(own8.at[0], d_send.at[4])
    await_bytes(yrel, ry_send.at[0])
    await_bytes(ysum, ry_send.at[1])
    await_bytes(ysum, ry_send.at[2])
    await_bytes(zrecv.at[pl.ds(0, nz - 1)], rz_sem.at[0])
    await_bytes(afull.at[0, pl.ds(0, nz - 1), 0], a_send.at[0])
    await_bytes(afull.at[0, :, pl.ds(0, ny - 1)], a_send.at[1])
    gather_close(gfull, 0)
    gather_close(pfull, 1)
    await_bytes(s1.at[pl.ds(0, 2 * nx - 1)], s_send.at[0])
    await_bytes(s2.at[pl.ds(0, nz - 1)], s_send.at[1])
    await_bytes(s3.at[pl.ds(0, ny - 1)], s_send.at[2])


def write_out(*refs):
    n = (len(refs) - 1) // 2
    sems = refs[-1]
    copies = [pltpu.make_async_copy(refs[i], refs[n + i], sems.at[i]) for i in range(n)]
    for copy in copies:
        copy.start()
    for copy in copies:
        copy.wait()


def body(nz, ny, nx, gz, inputs, key_grads, weights, momentum, left_stat, right_stat, left_root, right_root):
    tokens, width = inputs.shape
    ng, blk, ngr = nz // gz, ny * ROWS, nz // 2 + 1
    dma = pltpu.SemaphoreType.DMA
    v = pltpu.VMEM
    scratch = [
        v((ng, tokens, gz * blk), BF16), v((tokens, 2 * H), BF16), v((2 * H, tokens), BF16),
        v((ng, 2, gz, H, blk), F32), v((ng, gz, H, blk), F32),
        v((nz, ny, ROWS, H), F32), v((ny, nz, ROWS, H), BF16),
        v((3, nz, ROWS, H), BF16), v((2, nz, ROWS, H), BF16), v((4, nz, ROWS, H), BF16),
        v((nz, ROWS, H), F32), v((nz, ROWS, H), F32),
        v((2, nz, ny, ROWS, H), BF16), v((2, width, H), BF16), v((2, nz, ny, ROWS, H), BF16), v((2, nz, ny, ROWS, H), F32),
        v((2, 8, H), F32), v((ROWS, H), F32), v((2, 8, H), F32), v((ROWS, H), F32),
        v((8, 2 * H), F32), v((8, 2 * H), F32), v((8, width), F32), v((2, H, H), F32), v((2, 8, width), BF16), v((2, H, H), BF16),
        v((2, H), F32), v((2 * nx, 2, H), F32), v((nz, 2, H), F32), v((ny, 2, H), F32),
        pltpu.SemaphoreType.REGULAR, dma((7,)), dma((ng,)), dma((5,)), dma((ng + 4,)), dma((3,)), dma((ng,)), dma((ng,)), dma((2,)), dma((2,)), dma((7,)),
        dma((2, 3)), dma((2, ngr)), dma((2, ngr)), dma((2, ngr)), dma((2, ngr)), dma((3,)), dma((3,)),
    ]
    sds = jax.ShapeDtypeStruct
    anyspace = pl.BlockSpec(memory_space=pl.ANY)
    local = pl.BlockSpec(memory_space=pltpu.VMEM)
    shapes = (
        (weights.shape, F32), ((8, width), F32), (right_stat.shape, F32),
        (weights.shape, F32), (weights.shape, F32), ((width, 2 * H), BF16),
    )
    held = pl.pallas_call(
        functools.partial(kernel, nz, ny, nx, gz),
        out_shape=tuple(HELD(*s) for s in shapes),
        in_specs=[anyspace] * 8,
        out_specs=(local,) * 6,
        scratch_shapes=scratch,
        compiler_params=pltpu.CompilerParams(collective_id=0, has_side_effects=True, vmem_limit_bytes=56 * 2**20),
    )(inputs, key_grads, weights, momentum, left_stat, right_stat, left_root, right_root)
    mom, left, right, upd, nxt, copy = pl.pallas_call(
        write_out,
        out_shape=tuple(sds(*s) for s in shapes),
        in_specs=[local] * 6,
        out_specs=(anyspace,) * 6,
        scratch_shapes=[dma((6,))],
    )(*(pltpu.with_memory_space_constraint(h, pltpu.VMEM) for h in held))
    return mom, left[None], right, upd, nxt, copy


def build(devices, nz, ny, nx, gz):
    split = Mesh(devices.reshape(nz, ny, 2, nx), ("z", "y", "c", "x"))
    fs = ("z", "y", "c")
    in_specs = (
        P(fs, None), P(fs, "x"), P(fs, "x"), P(fs, "x"),
        P("x", fs, None), P("x", None, None), P("x", fs, None), P("x", None, None),
    )
    out_specs = (P(fs, "x"), P("x", fs, None), P("x", None, None), P(fs, "x"), P(fs, "x"), P(None, "x"))
    return jax.shard_map(
        functools.partial(body, nz, ny, nx, gz), mesh=split, in_specs=in_specs, out_specs=out_specs, check_vma=False
    )


def solution(mesh):
    return build(mesh.devices, 16, 8, mesh.shape["tp"], 4)
```

```python
import functools

import jax
import jax.numpy as jnp
from jax import lax
from jax.experimental import pallas as pl
from jax.experimental.pallas import tpu as pltpu
from jax.sharding import Mesh
from jax.sharding import PartitionSpec as P

MESH = pl.DeviceIdType.MESH
F32 = jnp.float32
BF16 = jnp.bfloat16
H = 128
ROWS = 16


def offset_of(r, nz):
    half = nz // 2
    if r == 0:
        return half
    return half - (r + 1) // 2 if r % 2 else -(half - r // 2)


def place_of(off, nz):
    half = nz // 2
    if off == 0:
        return nz - 1
    if abs(off) == half:
        return 0
    return 2 * (half - off) - 1 if off > 0 else 2 * (half + off)


HELD = pltpu.VMEM


def kernel(
    nz, ny, nx, gz,
    x_hbm, k_hbm, w_hbm, m_hbm, ls_hbm, rs_hbm, lr_hbm, rr_hbm,
    momv, lnv, rnv, upv, wnv, outv,
    xs, ks, kt, pt, px, sf, ysend, yrel, ysum, yrecv, zsend, zrecv, gfull, gabs, pfull, afull, ascr, tile, own8, gown,
    wv, mv, lsv, rsv, lrv, rrv,
    sv, s1, s2, s3,
    hello, in_sem, x_sem, d_send, d_recv, ry_send, rel_recv, ry_recv, rz_sem, a_send, a_recv,
    ag_send, agz_recv, agx_recv, agy_recv, agd_recv, s_send, s_recv,
):
    ng = nz // gz
    blk = ny * ROWS
    half = nz // 2
    z, y, c, x = (lax.axis_index(n) for n in ("z", "y", "c", "x"))
    me = nz - 1
    other = 1 - c
    sgn = 1 - 2 * c
    partner = {"c": other}
    quad, zi = z // gz, lax.rem(z, gz)
    my8 = pl.ds(pl.multiple_of(8 * c, 8), 8)
    its8 = pl.ds(pl.multiple_of(8 * other, 8), 8)

    def zpos(off):
        return lax.rem(z + off + nz, nz)

    def ypos(dy):
        return lax.rem(y + dy + ny, ny)

    def send(src, dst, s, r, dev):
        pltpu.make_async_remote_copy(src, dst, s, r, device_id=dev, device_id_type=MESH).start()

    def await_bytes(ref, sem):
        pltpu.make_async_copy(ref, ref, sem).wait()

    xc_peers = [(dx, dc) for dx in range(nx) for dc in range(2) if dx or dc]

    def xc_dev(dx, dc):
        return {"x": lax.rem(x + dx, nx), "c": lax.rem(c + dc, 2)}

    def load(src, dst, i):
        pltpu.make_async_copy(src, dst, in_sem.at[i]).start()

    def loaded(dst, i):
        await_bytes(dst, in_sem.at[i])

    quads = [offset_of(r, ng) for r in range(ng)] if ng > 1 else [0]

    def quad_of(g):
        return lax.rem(quad + quads[g] + ng, ng)

    load(k_hbm, ks, 0)
    for g in range(ng):
        src = x_hbm.at[:, pl.ds(pl.multiple_of(quad_of(g) * (gz * blk), gz * blk), gz * blk)]
        pltpu.make_async_copy(src, xs.at[g], x_sem.at[g]).start()
    load(w_hbm, wv, 1)
    load(m_hbm, mv, 2)
    load(lr_hbm.at[0], lrv.at[c], 3)
    load(rr_hbm, rrv, 4)
    load(ls_hbm.at[0], lsv, 5)
    load(rs_hbm, rsv, 6)

    bar = pltpu.get_barrier_semaphore()
    for dx, dc in xc_peers:
        pl.semaphore_signal(bar, inc=1, device_id=xc_dev(dx, dc), device_id_type=MESH)

    @pl.loop(1, ny)
    def _(dy):
        pl.semaphore_signal(bar, inc=1, device_id={"y": ypos(dy)}, device_id_type=MESH)

    near = sorted({d % nz for d in range(-4, 5) if d % nz})
    for dz in near:
        pl.semaphore_signal(bar, inc=1, device_id={"z": lax.rem(z + dz, nz)}, device_id_type=MESH)

    def matmul(g):
        await_bytes(xs.at[g], x_sem.at[g])
        out = jnp.dot(kt[...], xs[g], preferred_element_type=F32)
        for i in range(gz):
            for h in range(2):
                pt[g, h, i] = out[h * H:(h + 1) * H, i * blk:(i + 1) * blk]

    def exchange(g):
        send(pt.at[g, other], px.at[g], d_send.at[0], d_recv.at[g], partner)

    def span(g):
        return pl.ds(g * gz, gz)

    def scatter_y(g):
        await_bytes(px.at[g], d_recv.at[g])
        for i in range(gz):
            r = g * gz + i
            t = (pt[g, c, i] + px[g, i]).T.reshape(ny, ROWS, H)
            sf[r] = t
            ysend[:, r] = t.astype(BF16)
        for dst, via, slot in ((ypos(4), 2 * sgn, 2), (ypos(3), 1, 0), (ypos(-3), -1, 1)):
            send(ysend.at[dst, span(g)], yrel.at[slot, span(g)], ry_send.at[0], rel_recv.at[g], {"y": ypos(via)})
        for d, slot in ((1, 0), (-1, 1)):
            send(ysend.at[ypos(d), span(g)], yrecv.at[slot, span(g)], ry_send.at[1], ry_recv.at[g], {"y": ypos(d)})

    loaded(ks, 0)
    kt[...] = ks[...].T
    matmul(0)
    loaded(wv, 1)
    loaded(mv, 2)
    base = 0.9 * wv[...] - 0.225 * mv[...]
    ascr[0] = base[:, :H]
    ascr[1] = base[:, H:]
    afull[c, me, y, my8] = ascr[c]
    loaded(lrv.at[c], 3)

    pl.semaphore_wait(bar, (ny - 1) + len(near) + len(xc_peers))
    far = len(near) < nz - 1
    if far:
        for dz in (4, -4):
            pl.semaphore_signal(hello, inc=1, device_id={"z": zpos(dz)}, device_id_type=MESH)

    exchange(0)
    send(ascr.at[other], afull.at[other, me, y, my8], d_send.at[1], d_recv.at[ng], partner)
    send(lrv.at[c], lrv.at[c], d_send.at[2], d_recv.at[ng + 1], partner)
    up_mask = (1 - c).astype(F32)
    down_mask = c.astype(F32)

    def relay_y(g):
        await_bytes(yrel.at[:, span(g)], rel_recv.at[g])
        for i in range(gz):
            r = g * gz + i
            far = yrel[2, r].astype(F32)
            ysum[0, r] = (sf[r, ypos(2)] + yrel[0, r].astype(F32) + up_mask * far).astype(BF16)
            ysum[1, r] = (sf[r, ypos(-2)] + yrel[1, r].astype(F32) + down_mask * far).astype(BF16)
        for d, slot in ((2, 0), (-2, 1)):
            send(ysum.at[slot, span(g)], yrecv.at[2 + slot, span(g)], ry_send.at[2], ry_recv.at[g], {"y": ypos(d)})

    def scatter_z(g):
        await_bytes(yrecv.at[:, span(g)], ry_recv.at[g])
        for i in range(gz):
            r = g * gz + i
            t = sf[r, y]
            for j in range(4):
                t = t + yrecv[j, r].astype(F32)
            zsend[r] = t
        for i in range(gz):
            if quads[g]:
                send(zsend.at[g * gz + i], zrecv.at[z], rz_sem.at[0], rz_sem.at[1], {"z": quad_of(g) * gz + i})
            elif i:
                at = lax.rem(zi + i, gz)
                send(zsend.at[g * gz + at], zrecv.at[z], rz_sem.at[0], rz_sem.at[1], {"z": quad * gz + at})

    pieces = ((0, half), (half, nz - half))

    def base_z(is_near):
        if is_near:
            await_bytes(ascr.at[0], d_recv.at[ng])
        elif far:
            pl.semaphore_wait(hello, 2)
        for r in range(nz - 1):
            off = offset_of(r, nz)
            if (off % nz in near) != is_near:
                continue
            send(afull.at[c, me, y], afull.at[c, place_of(-off, nz), y], a_send.at[0], a_recv.at[0], {"z": zpos(off)})

    def base_y(p):
        r0, n = pieces[p]
        if p == 0:
            await_bytes(afull.at[c, pl.ds(0, nz - 1), y], a_recv.at[0])
        slab = afull.at[c, pl.ds(r0, n), y]
        for d in (2, -2):
            send(slab, slab, a_send.at[1], a_recv.at[1 + p], {"y": ypos(d)})
        for d in (1, -1):
            send(slab, slab, a_send.at[1], a_recv.at[3 + p], {"y": ypos(d)})

    def base_relay(p):
        r0, n = pieces[p]
        await_bytes(afull.at[c, pl.ds(r0, n), pl.ds(0, 2)], a_recv.at[1 + p])
        for origin, to in ((-2 * sgn, 2 * sgn), (-2, 1), (2, -1)):
            slab = afull.at[c, pl.ds(r0, n), ypos(origin)]
            send(slab, slab, a_send.at[1], a_recv.at[3 + p], {"y": ypos(to)})

    def base_land(p):
        r0, n = pieces[p]
        await_bytes(afull.at[c, pl.ds(r0, n), pl.ds(0, 5)], a_recv.at[3 + p])
        slab = afull.at[c, pl.ds(r0, n)]
        send(slab, slab, d_send.at[3], a_recv.at[5 + p], partner)

    for g in range(1, ng):
        matmul(g)
        exchange(g)
        scatter_y(g - 1)
        if g == 1:
            base_z(True)
    if ng == 1:
        base_z(True)
    base_z(False)
    early = min(2, ng - 1)
    if early:
        relay_y(0)
    scatter_y(ng - 1)
    for g in range(1 if early else 0, ng - 1):
        relay_y(g)
    if ng > 1:
        scatter_z(0)
    relay_y(ng - 1)
    for g in range(1 if ng > 1 else 0, ng):
        scatter_z(g)
    zrecv[z] = zsend[(ng - 1) * gz + zi]
    base_y(0)
    base_y(1)

    await_bytes(zrecv.at[pl.ds(0, nz - 1)], rz_sem.at[1])
    grad = zrecv[0]
    for r in range(1, nz):
        grad = grad + zrecv[r]
    sv[0:1] = jnp.sum(grad * grad, axis=0, keepdims=True)
    gfull[c, me, y] = grad.astype(BF16)

    groups = [(me, 1), (13, 2), (9, 4), (5, 4), (1, 4), (0, 1)] if nz == 16 else [(me, 1)] + [(r, 2) for r in range(nz - 3, 0, -2)] + [(0, 1)]
    ngr = len(groups)
    lag = min(3, ngr - 1)
    direct = range(max(ngr - 1, 1), ngr)

    def gather_start(full, p):
        order = [*range(nz - 3, nz - 1), *range(nz - 3)] if nz > 2 else [0]
        for r in order:
            off = offset_of(r, nz)
            back = place_of(-off, nz)
            j = [q for q, (r0, n) in enumerate(groups) if r0 <= back < r0 + n][0]
            send(full.at[c, me, y], full.at[c, back, y], ag_send.at[p, 0], agz_recv.at[p, j], {"z": zpos(off)})
        gather_forward(full, p, 0)

    def gather_forward(full, p, j):
        r0, n = groups[j]
        if j:
            await_bytes(full.at[c, pl.ds(r0, n), y], agz_recv.at[p, j])
        slab = full.at[c, pl.ds(r0, n), y]
        if j in direct:
            for d in (4, 3, -3, 2, -2, 1, -1):
                send(slab, slab, ag_send.at[p, 1], agy_recv.at[p, j], {"y": ypos(d)})
            return
        for d in (2, -2):
            send(slab, slab, ag_send.at[p, 1], agx_recv.at[p, j], {"y": ypos(d)})
        for d in (1, -1):
            send(slab, slab, ag_send.at[p, 1], agy_recv.at[p, j], {"y": ypos(d)})

    def gather_relay(full, p, j):
        if j in direct:
            return
        r0, n = groups[j]
        await_bytes(full.at[c, pl.ds(r0, n), pl.ds(0, 2)], agx_recv.at[p, j])
        for origin, to in ((-2 * sgn, 2 * sgn), (-2, 1), (2, -1)):
            slab = full.at[c, pl.ds(r0, n), ypos(origin)]
            send(slab, slab, ag_send.at[p, 1], agy_recv.at[p, j], {"y": ypos(to)})

    def gather_land(full, p, j):
        r0, n = groups[j]
        await_bytes(full.at[c, pl.ds(r0, n), pl.ds(0, ny - 1 if j in direct else 5)], agy_recv.at[p, j])
        slab = full.at[c, pl.ds(r0, n)]
        send(slab, slab, ag_send.at[p, 2], agd_recv.at[p, j], partner)

    def gather(full, p, after_forward, before_land, after_land):
        for j in range(1, ngr):
            gather_forward(full, p, j)
            after_forward(j)
            if j >= lag:
                gather_relay(full, p, j - lag)
        for j in range(ngr - lag, ngr):
            gather_relay(full, p, j)
        before_land()
        for j in range(ngr):
            gather_land(full, p, j)
            after_land(j)

    def gather_close(full, p):
        await_bytes(full.at[0, pl.ds(0, nz - 1), 0], ag_send.at[p, 0])
        await_bytes(full.at[0, :, pl.ds(0, ny - 1)], ag_send.at[p, 1])
        await_bytes(full.at[0], ag_send.at[p, 2])

    def keep(h, j):
        r0, n = groups[j]
        for r in range(r0, r0 + n):
            gabs[h, pl.ds(pl.multiple_of(zpos(offset_of(r, nz)) * blk, blk), blk)] = gfull[h, r].reshape(blk, H)

    gather_start(gfull, 0)
    gather(gfull, 0, lambda j: None, lambda: None, lambda j: keep(c, j))

    await_bytes(lrv.at[0], d_recv.at[ng + 1])
    loaded(rrv, 4)
    lm = jnp.concatenate([lrv[0].astype(F32), lrv[1].astype(F32)], axis=0).astype(BF16)
    left = jnp.dot(lm, gabs[c], preferred_element_type=F32)
    hi = left.astype(BF16)
    lo = (left - hi.astype(F32)).astype(BF16)
    rr = rrv[c]
    pre = jnp.dot(hi, rr, preferred_element_type=F32) + jnp.dot(lo, rr, preferred_element_type=F32)
    pfull[c, me, y] = pre.astype(BF16)
    gather_start(pfull, 1)
    sv[1:2] = jnp.sum(pre * pre, axis=0, keepdims=True)
    tile[...] = pre

    s3[y] = sv[...]

    @pl.loop(1, ny)
    def _(dy):
        send(sv, s3.at[y], s_send.at[2], s_recv.at[2], {"y": ypos(dy)})

    for p in range(2):
        base_relay(p)
    send(tile.at[its8], own8.at[c], d_send.at[4], d_recv.at[ng + 3], partner)
    own8[c] = tile[my8]

    def total(buf, n):
        tot = buf[0]
        for i in range(1, n):
            tot = tot + buf[i]
        return tot

    await_bytes(s3.at[pl.ds(0, ny - 1)], s_recv.at[2])
    s2[z] = total(s3, ny)

    @pl.loop(1, nz)
    def _(dz):
        send(s2.at[z], s2.at[z], s_send.at[1], s_recv.at[1], {"z": lax.rem(z + dz, nz)})

    def before_land():
        for j in range(ngr):
            r0, n = groups[j]
            await_bytes(gfull.at[other, pl.ds(r0, n)], agd_recv.at[0, j])
            keep(other, j)
        gram = None
        for h in range(2):
            gown[...] = gfull[h, me, y].astype(F32)
            part = lax.dot_general(
                gown[my8].astype(BF16), gabs[h], (((1,), (1,)), ((), ())), preferred_element_type=F32
            )
            gram = part if gram is None else gram + part
        loaded(lsv, 5)
        lnv[...] = 0.95 * lsv[...] + 0.05 * gram
        loaded(rsv, 6)
        for h in range(2):
            gh = gabs[h]
            hg = lax.dot_general(gh, gh, (((0,), (0,)), ((), ())), preferred_element_type=F32)
            rnv[h] = 0.95 * rsv[h] + 0.05 * hg
        for p in range(2):
            base_land(p)
        await_bytes(s2.at[pl.ds(0, nz - 1)], s_recv.at[1])
        s1[x * 2 + c] = total(s2, nz)
        for dx, dc in xc_peers:
            send(s1.at[x * 2 + c], s1.at[x * 2 + c], s_send.at[0], s_recv.at[0], xc_dev(dx, dc))

    gather(pfull, 1, lambda j: None, before_land, lambda j: None)

    await_bytes(s1.at[pl.ds(0, 2 * nx - 1)], s_recv.at[0])
    tot = total(s1, 2 * nx)
    gs = jnp.sum(tot[0:1], axis=1, keepdims=True)
    ps = jnp.sum(tot[1:2], axis=1, keepdims=True)
    scale = jnp.sqrt(gs / (ps + 1e-06))

    await_bytes(own8.at[0], d_recv.at[ng + 3])
    wide = jnp.concatenate([own8[0], own8[1]], axis=1)
    mom = 0.9 * mv[...] + scale * wide
    upd = -0.25 * (mom + 0.4 * wv[...])
    momv[...] = mom
    upv[...] = upd
    wnv[...] = wv[...] + upd

    for p in range(2):
        await_bytes(afull.at[other, pl.ds(*pieces[p])], a_recv.at[5 + p])
    quarter = 0.25 * scale
    for j in range(ngr):
        r0, n = groups[j]
        await_bytes(pfull.at[other, pl.ds(r0, n)], agd_recv.at[1, j])
        for r in range(r0, r0 + n):
            rows = pl.ds(pl.multiple_of(zpos(offset_of(r, nz)) * blk, blk), blk)
            for h in range(2):
                v = afull[h, r].reshape(blk, H) - quarter * pfull[h, r].reshape(blk, H).astype(F32)
                outv[rows, h * H:(h + 1) * H] = v.astype(BF16)

    await_bytes(pt.at[:, 0], d_send.at[0])
    await_bytes(ascr.at[0], d_send.at[1])
    await_bytes(lrv.at[0], d_send.at[2])
    await_bytes(afull.at[0], d_send.at[3])
    await_bytes(own8.at[0], d_send.at[4])
    await_bytes(yrel, ry_send.at[0])
    await_bytes(ysum, ry_send.at[1])
    await_bytes(ysum, ry_send.at[2])
    await_bytes(zrecv.at[pl.ds(0, nz - 1)], rz_sem.at[0])
    await_bytes(afull.at[0, pl.ds(0, nz - 1), 0], a_send.at[0])
    await_bytes(afull.at[0, :, pl.ds(0, ny - 1)], a_send.at[1])
    gather_close(gfull, 0)
    gather_close(pfull, 1)
    await_bytes(s1.at[pl.ds(0, 2 * nx - 1)], s_send.at[0])
    await_bytes(s2.at[pl.ds(0, nz - 1)], s_send.at[1])
    await_bytes(s3.at[pl.ds(0, ny - 1)], s_send.at[2])


def write_out(*refs):
    n = (len(refs) - 1) // 2
    sems = refs[-1]
    copies = [pltpu.make_async_copy(refs[i], refs[n + i], sems.at[i]) for i in range(n)]
    for copy in copies:
        copy.start()
    for copy in copies:
        copy.wait()


def body(nz, ny, nx, gz, inputs, key_grads, weights, momentum, left_stat, right_stat, left_root, right_root):
    tokens, width = inputs.shape
    ng, blk, ngr = nz // gz, ny * ROWS, nz // 2 + 1
    dma = pltpu.SemaphoreType.DMA
    v = pltpu.VMEM
    scratch = [
        v((ng, tokens, gz * blk), BF16), v((tokens, 2 * H), BF16), v((2 * H, tokens), BF16),
        v((ng, 2, gz, H, blk), F32), v((ng, gz, H, blk), F32),
        v((nz, ny, ROWS, H), F32), v((ny, nz, ROWS, H), BF16),
        v((3, nz, ROWS, H), BF16), v((2, nz, ROWS, H), BF16), v((4, nz, ROWS, H), BF16),
        v((nz, ROWS, H), F32), v((nz, ROWS, H), F32),
        v((2, nz, ny, ROWS, H), BF16), v((2, width, H), BF16), v((2, nz, ny, ROWS, H), BF16), v((2, nz, ny, ROWS, H), F32),
        v((2, 8, H), F32), v((ROWS, H), F32), v((2, 8, H), F32), v((ROWS, H), F32),
        v((8, 2 * H), F32), v((8, 2 * H), F32), v((8, width), F32), v((2, H, H), F32), v((2, 8, width), BF16), v((2, H, H), BF16),
        v((2, H), F32), v((2 * nx, 2, H), F32), v((nz, 2, H), F32), v((ny, 2, H), F32),
        pltpu.SemaphoreType.REGULAR, dma((7,)), dma((ng,)), dma((5,)), dma((ng + 4,)), dma((3,)), dma((ng,)), dma((ng,)), dma((2,)), dma((2,)), dma((7,)),
        dma((2, 3)), dma((2, ngr)), dma((2, ngr)), dma((2, ngr)), dma((2, ngr)), dma((3,)), dma((3,)),
    ]
    sds = jax.ShapeDtypeStruct
    anyspace = pl.BlockSpec(memory_space=pl.ANY)
    local = pl.BlockSpec(memory_space=pltpu.VMEM)
    shapes = (
        (weights.shape, F32), ((8, width), F32), (right_stat.shape, F32),
        (weights.shape, F32), (weights.shape, F32), ((width, 2 * H), BF16),
    )
    held = pl.pallas_call(
        functools.partial(kernel, nz, ny, nx, gz),
        out_shape=tuple(HELD(*s) for s in shapes),
        in_specs=[anyspace] * 8,
        out_specs=(local,) * 6,
        scratch_shapes=scratch,
        compiler_params=pltpu.CompilerParams(collective_id=0, has_side_effects=True, vmem_limit_bytes=56 * 2**20),
    )(inputs, key_grads, weights, momentum, left_stat, right_stat, left_root, right_root)
    mom, left, right, upd, nxt, copy = pl.pallas_call(
        write_out,
        out_shape=tuple(sds(*s) for s in shapes),
        in_specs=[local] * 6,
        out_specs=(anyspace,) * 6,
        scratch_shapes=[dma((6,))],
    )(*(pltpu.with_memory_space_constraint(h, pltpu.VMEM) for h in held))
    return mom, left[None], right, upd, nxt, copy


def build(devices, nz, ny, nx, gz):
    split = Mesh(devices.reshape(nz, ny, 2, nx), ("z", "y", "c", "x"))
    fs = ("z", "y", "c")
    in_specs = (
        P(fs, None), P(fs, "x"), P(fs, "x"), P(fs, "x"),
        P("x", fs, None), P("x", None, None), P("x", fs, None), P("x", None, None),
    )
    out_specs = (P(fs, "x"), P("x", fs, None), P("x", None, None), P(fs, "x"), P(fs, "x"), P(None, "x"))
    return jax.shard_map(
        functools.partial(body, nz, ny, nx, gz), mesh=split, in_specs=in_specs, out_specs=out_specs, check_vma=False
    )


def solution(mesh):
    return build(mesh.devices, 16, 8, mesh.shape["tp"], 4)
```
